32 devices in a mesh: grp: 2 (over y), sp: 4 (over z), tp: 4 (over x, core).
Axes of the slice: x: 2, y: 2, z: 4, core: 2. Of those that a mesh axis runs over, the one named last changes fastest.
Arguments:
- query_rows: bfloat16 [1024, 1024], P(('grp', 'sp'), 'tp'), parts along dimension 0, may hold values from -12 to 12
- key_rows: bfloat16 [1024, 1024], P(('grp', 'sp'), 'tp'), parts along dimension 0, may hold values from -9 to 9
- value_rows: bfloat16 [1024, 1024], P(('grp', 'sp'), 'tp'), parts along dimension 0, may hold values from -6 to 6
- key_logit: bfloat16 [1024, 8], P(('grp', 'sp'), 'tp'), parts along dimension 0, as said below
- residual: bfloat16 [1024, 2048], P(('grp', 'sp')), parts along dimension 0, may hold values from -6 to 6
- out_weight: bfloat16 [1024, 2048], P('tp'), may hold values from -0.1875 to 0.1875
- mix_gain: float32 [2048], replicated, may hold values from 0.1 to 1.9
- ffn_gain: float32 [2048], replicated, may hold values from 0.1 to 1.9
- out_gain: float32 [2048], replicated, may hold values from 0.1 to 1.9
- gate_weight: bfloat16 [2048, 5120], P('sp', 'tp'), may hold values from -0.125 to 0.125
- up_weight: bfloat16 [2048, 5120], P('sp', 'tp'), may hold values from -0.125 to 0.125
- down_weight: bfloat16 [2048, 5120], P('sp', 'tp'), may hold values from -0.078125 to 0.078125
Outputs:
- layer_out: bfloat16 [1024, 2048], P(('grp', 'sp')), parts along dimension 0
The draws below stay inside these ranges and needn't reach their ends.
There are 2 independent parts, one for each index of `grp`. The reference program is written for one: setup_inputs(seed, part) draws one part's arguments, and reference() takes and returns one part's arrays. A program takes and returns all parts, laid end to end along the dimension named above; an argument that names none is the same for every part. Nothing has to cross between parts.
Inputs may be any that keep to these rules, and one draw needn't show every extreme that they name: `key_logit`: log-odds offsets of the keys, all negative.
All inputs are finite; a program needn't handle non-finite values.
Results may differ from the reference program's by a relative error of at most 0.018.
Values may be sent and summed in bfloat16 or wider, within the bound.
No kernel may reach another device: no remote copies, remote signals or barrier semaphores. Data moves between devices by JAX's collectives and lax.ppermute only.
A program may use at most 64 MiB of HBM per device.

```python
import math
import jax
import jax.numpy as jnp
from jax import lax

D = 2048
ATTENTION_COUNT = 8
HEAD_DIM = 128
FF = 5120
TOK_DEV = 128
SEQUENCE_LENGTH = 512
HEAD_GROUP = 2
FF_GROUP = 1280
N_SP = 4
N_TP = 4


def draw_key_logit(key, part):
    flowing_entries = jax.random.split(key, 5)
    length_log = math.log(SEQUENCE_LENGTH)
    starting_shift = jax.random.uniform(flowing_entries[0], (ATTENTION_COUNT,), jnp.float32, -7.5 - length_log, -8.5)
    tile_spacing = jax.random.uniform(flowing_entries[1], (SEQUENCE_LENGTH // TOK_DEV, ATTENTION_COUNT), jnp.float32, -0.7, 0.7)
    tile_spacing = jnp.repeat(tile_spacing, TOK_DEV, axis=0)
    gaussian_perturbation = 0.3 * jax.random.normal(flowing_entries[2], (SEQUENCE_LENGTH, ATTENTION_COUNT), jnp.float32)
    spots = jax.random.randint(flowing_entries[3], (3, ATTENTION_COUNT), 0, SEQUENCE_LENGTH)
    places = jnp.arange(SEQUENCE_LENGTH, dtype=jnp.int32)[:, None, None]
    hit_entries = jnp.any(places == spots[None, :, :], axis=1)
    sudden_entries = jax.random.uniform(flowing_entries[4], (SEQUENCE_LENGTH, ATTENTION_COUNT), jnp.float32, -1.5, -0.5)
    payload_table = jnp.where(hit_entries, sudden_entries, starting_shift[None, :] + tile_spacing + gaussian_perturbation)
    return payload_table.astype(jnp.bfloat16)


def levels(own_key, shape, cuts, low, top_value):
    level, own = 1.0, jax.random.fold_in(own_key, 6)
    for dim, shards_of in cuts:
        draws = jnp.exp(jax.random.uniform(jax.random.fold_in(own, dim), (shards_of,), jnp.float32, low / len(cuts), top_value / len(cuts)))
        level = level * jnp.repeat(draws, shape[dim] // shards_of).reshape([-1 if axis == dim else 1 for axis in range(len(shape))])
    return level


def normal_values(key, dims, spread, reach, cuts=(), kind=jnp.bfloat16):
    array = spread * jax.random.normal(key, dims, jnp.float32)
    if cuts:
        array = array * levels(key, dims, cuts, -0.22, 0.18)
    return jnp.clip(array, -reach, reach).astype(kind)


def setup_inputs(seed: int = 0, part: int = 0) -> dict:
    key_list = jax.random.split(jax.random.key(seed), 13)
    part_keys = jax.random.split(jax.random.fold_in(key_list[12], part), 13)
    return {
        "query_rows": normal_values(part_keys[0], (SEQUENCE_LENGTH, ATTENTION_COUNT * HEAD_DIM), 2.0, 12.0, ((0, 4), (1, 4))),
        "key_rows": normal_values(part_keys[1], (SEQUENCE_LENGTH, ATTENTION_COUNT * HEAD_DIM), 1.5, 9.0, ((0, 4), (1, 4))),
        "value_rows": normal_values(part_keys[2], (SEQUENCE_LENGTH, ATTENTION_COUNT * HEAD_DIM), 1.0, 6.0, ((0, 4), (1, 4))),
        "key_logit": draw_key_logit(jax.random.fold_in(jax.random.fold_in(key_list[12], part), 71), part),
        "residual": normal_values(part_keys[4], (SEQUENCE_LENGTH, D), 1.0, 6.0, ((0, 4),)),
        "out_weight": normal_values(key_list[5], (ATTENTION_COUNT * HEAD_DIM, D), (ATTENTION_COUNT * HEAD_DIM) ** -0.5, 0.1875, ((0, 4),)),
        "mix_gain": jnp.clip(1.0 + 0.18 * jax.random.normal(key_list[6], (D,), jnp.float32), 0.1, 1.9),
        "ffn_gain": jnp.clip(1.0 + 0.18 * jax.random.normal(key_list[7], (D,), jnp.float32), 0.1, 1.9),
        "out_gain": jnp.clip(1.0 + 0.18 * jax.random.normal(key_list[8], (D,), jnp.float32), 0.1, 1.9),
        "gate_weight": normal_values(key_list[9], (D, FF), D ** -0.5, 0.125, ((0, 4), (1, 4))),
        "up_weight": normal_values(key_list[10], (D, FF), D ** -0.5, 0.125, ((0, 4), (1, 4))),
        "down_weight": normal_values(key_list[11], (D, FF), FF ** -0.5, 0.078125, ((0, 4), (1, 4))),
    }


epsilon = 1e-06

def normalize(payload_table):
    return payload_table * lax.rsqrt(lax.optimization_barrier(jnp.mean(payload_table * payload_table, axis=-1, keepdims=True)) + epsilon)

def block_terms(queries, key_part, value_part, logit_part, query_block, key_block):
    scores = jnp.einsum('hqd,khd->hqk', queries.astype(jnp.float32), key_part.astype(jnp.float32)) * HEAD_DIM ** (-0.5)
    scores = scores + jnp.transpose(logit_part.astype(jnp.float32))[:, None, :]
    query_pos = query_block * TOK_DEV + jnp.arange(TOK_DEV, dtype=jnp.int32)[:, None]
    key_pos = key_block * TOK_DEV + jnp.arange(TOK_DEV, dtype=jnp.int32)[None, :]
    causal = key_pos < query_pos
    keep_log = jnp.where(causal, jax.nn.log_sigmoid(-scores), 0.0)
    totals = lax.optimization_barrier(jnp.sum(keep_log, axis=2))
    within = lax.cumsum(keep_log, axis=2, reverse=True) - keep_log
    sticks = jnp.where(causal, jnp.exp(jax.nn.log_sigmoid(scores) + within), 0.0).astype(jnp.bfloat16)
    partials = jnp.einsum('hqk,khd->hqd', sticks.astype(jnp.float32), value_part.astype(jnp.float32))
    return (totals, partials)

def reference(query_rows, key_rows, value_rows, key_logit, residual, out_weight, mix_gain, ffn_gain, out_gain, gate_weight, up_weight, down_weight):

    def one_block(query_block):
        start = (query_block * TOK_DEV).astype(jnp.int32)
        queries = lax.dynamic_slice_in_dim(query_rows, start, TOK_DEV, 0).reshape(TOK_DEV, ATTENTION_COUNT, HEAD_DIM).transpose(1, 0, 2)

        def key_terms(key_block):
            key_start = (key_block * TOK_DEV).astype(jnp.int32)
            key_part = lax.dynamic_slice_in_dim(key_rows, key_start, TOK_DEV, 0).reshape(TOK_DEV, ATTENTION_COUNT, HEAD_DIM)
            value_part = lax.dynamic_slice_in_dim(value_rows, key_start, TOK_DEV, 0).reshape(TOK_DEV, ATTENTION_COUNT, HEAD_DIM)
            logit_part = lax.dynamic_slice_in_dim(key_logit, key_start, TOK_DEV, 0)

            def compute(unused):
                return block_terms(queries, key_part, value_part, logit_part, query_block, key_block)

            def skipped(unused):
                return (jnp.zeros((ATTENTION_COUNT, TOK_DEV), jnp.float32), jnp.zeros((ATTENTION_COUNT, TOK_DEV, HEAD_DIM), jnp.float32))
            return lax.cond(key_block <= query_block, compute, skipped, 0)
        totals, partials = lax.map(key_terms, jnp.arange(N_SP, dtype=jnp.int32))
        suffix = lax.cumsum(totals, axis=0, reverse=True) - totals
        attended = jnp.einsum('bhq,bhqd->qhd', jnp.exp(suffix), partials, precision=lax.Precision.HIGHEST)
        attended = attended.reshape(TOK_DEV, ATTENTION_COUNT * HEAD_DIM).astype(jnp.bfloat16)
        head_part = jnp.einsum('qgc,gcd->gqd', attended.reshape(TOK_DEV, N_TP, HEAD_GROUP * HEAD_DIM).astype(jnp.float32), out_weight.reshape(N_TP, HEAD_GROUP * HEAD_DIM, D).astype(jnp.float32)).astype(jnp.bfloat16)
        mixed_rows = lax.optimization_barrier(jnp.sum(head_part.astype(jnp.float32), axis=0)).astype(jnp.bfloat16)
        own_residual = lax.dynamic_slice_in_dim(residual, start, TOK_DEV, 0).astype(jnp.float32)
        middle = (own_residual + mix_gain * normalize(mixed_rows.astype(jnp.float32))).astype(jnp.bfloat16)
        normed = (ffn_gain * normalize(middle.astype(jnp.float32))).astype(jnp.bfloat16)
        gate_act = jnp.dot(normed, gate_weight, preferred_element_type=jnp.float32)
        up_act = jnp.dot(normed, up_weight, preferred_element_type=jnp.float32)
        hidden = (jax.nn.silu(gate_act) * up_act).astype(jnp.bfloat16)
        unit_part = jnp.einsum('qgf,dgf->gqd', hidden.reshape(TOK_DEV, N_TP, FF_GROUP).astype(jnp.float32), down_weight.reshape(D, N_TP, FF_GROUP).astype(jnp.float32)).astype(jnp.bfloat16)
        ffn_out = lax.optimization_barrier(jnp.sum(unit_part.astype(jnp.float32), axis=0)).astype(jnp.bfloat16)
        return (middle.astype(jnp.float32) + out_gain * normalize(ffn_out.astype(jnp.float32))).astype(jnp.bfloat16)
    blocks_out = lax.map(one_block, jnp.arange(N_SP, dtype=jnp.int32))
    return blocks_out.reshape(SEQUENCE_LENGTH, D)
```

```python
import jax
import jax.numpy as jnp
from jax import lax
from jax.sharding import PartitionSpec as P

epsilon = 1e-06


def normalize(payload_table):
    return payload_table * lax.rsqrt(
        jnp.mean(payload_table * payload_table, axis=-1, keepdims=True) + epsilon
    )


def shift(rows, axis, step):
    count = lax.axis_size(axis)
    return lax.ppermute(rows, axis, [(i, (i + step) % count) for i in range(count)])


def upward(rows, axis, step):
    count = lax.axis_size(axis)
    return lax.ppermute(rows, axis, [(i, i + step) for i in range(count - step)])


def swap(rows, axis, bit):
    count = lax.axis_size(axis)
    return lax.ppermute(rows, axis, [(i, i ^ bit) for i in range(count)])


def spread(weight):
    ring, own = lax.axis_size("sp"), lax.axis_index("sp")
    copies, copy = lax.axis_size("grp"), lax.axis_index("grp")
    rows, columns = weight.shape
    part, share = columns // ring, rows // copies
    pieces = weight.reshape(rows, ring, part).transpose(1, 0, 2)
    result = jnp.zeros((ring * rows, part), weight.dtype)
    mine = lax.dynamic_index_in_dim(pieces, own, 0, keepdims=False)
    result = lax.dynamic_update_slice(result, mine, (own * rows, 0))
    for step in range(1, ring):
        target, source = (own + step) % ring, (own - step) % ring
        piece = lax.dynamic_slice(pieces, (target, copy * share, 0), (1, share, part))[0]
        piece = shift(piece, "sp", step)
        for turn in range(copies):
            other = piece if turn == 0 else shift(piece, "grp", turn)
            place = (copy - turn) % copies
            result = lax.dynamic_update_slice(result, other, (source * rows + place * share, 0))
    return result


def attend(queries, key_part, value_part, logit_part):
    tok_rows = queries.shape[0]
    head_count = logit_part.shape[1]
    head_width = queries.shape[1] // head_count
    ring = lax.axis_size("sp")
    queries = queries.reshape(tok_rows, head_count, head_width)
    position = jnp.arange(tok_rows, dtype=jnp.int32)
    later = (position[:, None] > position[None, :]).astype(jnp.float32)
    causal = ((position[:, None] > position[None, :])[None] | (jnp.arange(ring) > 0)[:, None, None])[:, None]
    packed = jnp.concatenate([key_part, value_part], axis=1)
    logit_rows = jnp.transpose(logit_part)
    blocks = jnp.stack([packed] + [upward(packed, "sp", step) for step in range(1, ring)])
    logits = jnp.stack([logit_rows] + [upward(logit_rows, "sp", step) for step in range(1, ring)])
    keys, values = jnp.split(blocks.reshape(ring, tok_rows, 2 * head_count, head_width), 2, axis=2)
    scores = jnp.einsum(
        "qhd,bkhd->bhqk", queries, keys, preferred_element_type=jnp.float32
    ) * head_width ** (-0.5)
    scores = scores + logits.astype(jnp.float32)[:, :, None, :]
    tail = jnp.log1p(jnp.exp(-jnp.abs(scores)))
    keep_log = jnp.where(causal, -jnp.maximum(scores, 0.0) - tail, 0.0)
    take_log = jnp.minimum(scores, 0.0) - tail
    within = jnp.einsum("bhqj,jk->bhqk", keep_log, later, precision=lax.Precision.HIGHEST)
    sticks = jnp.where(causal, jnp.exp(take_log + within), 0.0).astype(jnp.bfloat16)
    partials = jnp.einsum("bhqk,bkhd->bhqd", sticks, values, preferred_element_type=jnp.float32)
    totals = jnp.sum(keep_log, axis=3, keepdims=True)
    carried = jnp.cumsum(totals, axis=0) - totals
    attended = jnp.sum(jnp.exp(carried) * partials, axis=0)
    return (
        attended.transpose(1, 0, 2).reshape(tok_rows, head_count * head_width).astype(jnp.bfloat16)
    )


def shards(
    query_rows,
    key_rows,
    value_rows,
    key_logit,
    residual,
    out_weight,
    mix_gain,
    ffn_gain,
    out_gain,
    gate_weight,
    up_weight,
    down_weight,
):
    ring = lax.axis_size("sp")
    members, member = lax.axis_size("tp"), lax.axis_index("tp")
    tok_rows, width = residual.shape
    own_rows = tok_rows // members
    bits = [1 << i for i in range(members.bit_length() - 1)]

    attended = attend(query_rows, key_rows, value_rows, key_logit)
    gate_full, up_full, down_full = spread(gate_weight), spread(up_weight), spread(down_weight)

    head_part = jnp.dot(attended, out_weight, preferred_element_type=jnp.float32)
    head_part = head_part.astype(jnp.bfloat16).reshape(members, own_rows, width)
    mixed = jnp.zeros((own_rows, width), jnp.float32)
    for step in range(members):
        part = lax.dynamic_index_in_dim(head_part, member ^ step, 0, keepdims=False)
        part = part if step == 0 else swap(part, "tp", step)
        mixed = mixed + part.astype(jnp.float32)
    mixed = mixed.astype(jnp.bfloat16)
    own_residual = lax.dynamic_slice_in_dim(residual, member * own_rows, own_rows, 0)
    middle = (
        own_residual.astype(jnp.float32) + mix_gain * normalize(mixed.astype(jnp.float32))
    ).astype(jnp.bfloat16)
    normed = (ffn_gain * normalize(middle.astype(jnp.float32))).astype(jnp.bfloat16)

    gathered = jnp.stack(
        [normed if step == 0 else shift(normed, "sp", step) for step in range(ring)]
    )[None]
    for bit in reversed(bits):
        gathered = jnp.concatenate([gathered, swap(gathered, "tp", bit)], axis=0)
    gathered = gathered.reshape(members * ring * own_rows, width)

    gate_act = jnp.dot(gathered, gate_full, preferred_element_type=jnp.float32)
    up_act = jnp.dot(gathered, up_full, preferred_element_type=jnp.float32)
    hidden = (jax.nn.silu(gate_act) * up_act).astype(jnp.bfloat16)
    unit_part = lax.dot_general(
        hidden, down_full, (((1,), (1,)), ((), ())), preferred_element_type=jnp.float32
    ).astype(jnp.bfloat16)
    unit_part = unit_part.reshape(members, ring, own_rows, width)
    for bit in bits:
        kept, sent = jnp.split(unit_part, 2, axis=0)
        unit_part = (
            kept.astype(jnp.float32) + swap(sent, "tp", bit).astype(jnp.float32)
        ).astype(jnp.bfloat16)
    unit_part = unit_part[0]
    ffn_out = unit_part[0].astype(jnp.float32)
    for step in range(1, ring):
        ffn_out = ffn_out + shift(unit_part[step], "sp", -step).astype(jnp.float32)
    ffn_out = ffn_out.astype(jnp.bfloat16)
    layer_out = (
        middle.astype(jnp.float32) + out_gain * normalize(ffn_out.astype(jnp.float32))
    ).astype(jnp.bfloat16)
    block = layer_out[None]
    for bit in reversed(bits):
        block = jnp.concatenate([block, swap(block, "tp", bit)], axis=0)
    result = jnp.zeros((tok_rows, width), jnp.bfloat16)
    order = [0]
    for bit in reversed(bits):
        order = order + [o ^ bit for o in order]
    for slot, offset in enumerate(order):
        result = lax.dynamic_update_slice(
            result, block[slot], ((member ^ offset) * own_rows, 0)
        )
    return result


def solution(mesh):
    placed = (
        P(("grp", "sp"), "tp"),
        P(("grp", "sp"), "tp"),
        P(("grp", "sp"), "tp"),
        P(("grp", "sp"), "tp"),
        P(("grp", "sp"), None),
        P("tp", None),
        P(),
        P(),
        P(),
        P("sp", "tp"),
        P("sp", "tp"),
        P("sp", "tp"),
    )
    return jax.shard_map(
        shards, mesh=mesh, in_specs=placed, out_specs=P(("grp", "sp"), None), check_vma=False
    )
```

```python
import functools

import jax
import jax.numpy as jnp
from jax import lax
from jax.experimental import pallas as pl
from jax.experimental.pallas import tpu as pltpu
from jax.sharding import PartitionSpec as P

epsilon = 1e-06
lanes = 128
pad_rows = 16


def normalize(payload_table):
    return payload_table * lax.rsqrt(
        jnp.mean(payload_table * payload_table, axis=-1, keepdims=True) + epsilon
    )


def shift(rows, axis, step):
    count = lax.axis_size(axis)
    return lax.ppermute(rows, axis, [(i, (i + step) % count) for i in range(count)])


def upward(rows, axis, step):
    count = lax.axis_size(axis)
    return lax.ppermute(rows, axis, [(i, i + step) for i in range(count - step)])


def swap(rows, axis, bit):
    count = lax.axis_size(axis)
    return lax.ppermute(rows, axis, [(i, i ^ bit) for i in range(count)])


def call(kernel, name, outs, flops, *args, scalars=0, scratch=(), limit=None):
    specs = [pl.BlockSpec(memory_space=pltpu.SMEM)] * scalars
    specs += [pl.BlockSpec(memory_space=pltpu.VMEM)] * (len(args) - scalars)
    single = not isinstance(outs, list)
    out_list = [outs] if single else outs
    moved = sum(a.size * a.dtype.itemsize for a in (*args, *out_list))
    out_specs = [pl.BlockSpec(memory_space=pltpu.VMEM)] * len(out_list)
    return pl.pallas_call(
        kernel,
        name=name,
        out_shape=outs,
        in_specs=specs,
        out_specs=out_specs[0] if single else out_specs,
        scratch_shapes=list(scratch),
        compiler_params=pltpu.CompilerParams(vmem_limit_bytes=limit),
        cost_estimate=pl.CostEstimate(flops=flops, bytes_accessed=moved, transcendentals=0),
    )(*args)


def dot_t(a, b):
    return lax.dot_general(a, b, (((1,), (1,)), ((), ())), preferred_element_type=jnp.float32)


def pack_kernel(key_ref, value_ref, logit_ref, out_ref):
    tok_rows, width = key_ref.shape
    out_ref[:tok_rows, :width] = key_ref[...]
    out_ref[:tok_rows, width:] = value_ref[...]
    out_ref[tok_rows:, :tok_rows] = logit_ref[...]
    out_ref[tok_rows:, tok_rows:] = jnp.zeros((pad_rows, 2 * width - tok_rows), out_ref.dtype)


def attend_kernel(head_count, query_ref, *refs):
    blocks, out_ref = refs[:-1], refs[-1]
    tok_rows, width = query_ref.shape
    head_width = width // head_count
    row = lax.broadcasted_iota(jnp.int32, (tok_rows, tok_rows), 0)
    column = lax.broadcasted_iota(jnp.int32, (tok_rows, tok_rows), 1)
    causal = row > column
    later = causal.astype(jnp.float32).astype(jnp.bfloat16)
    for head in range(head_count):
        own = slice(head * head_width, (head + 1) * head_width)
        queries = query_ref[:, own]
        attended = jnp.zeros((tok_rows, head_width), jnp.float32)
        carried = jnp.zeros((tok_rows, 1), jnp.float32)
        for step, block in enumerate(blocks):
            keys = block[:tok_rows, own]
            values = block[:tok_rows, width + head * head_width : width + (head + 1) * head_width]
            logit = block[tok_rows:, :tok_rows].astype(jnp.float32)[head : head + 1]
            scores = dot_t(queries, keys) * head_width ** (-0.5) + logit
            tail = jnp.log(1.0 + jnp.exp(-jnp.abs(scores)))
            keep_log = -jnp.maximum(scores, 0.0) - tail
            take_log = jnp.minimum(scores, 0.0) - tail
            if step == 0:
                keep_log = jnp.where(causal, keep_log, 0.0)
            high = keep_log.astype(jnp.bfloat16)
            rest = keep_log - high.astype(jnp.float32)
            middle = rest.astype(jnp.bfloat16)
            low = (rest - middle.astype(jnp.float32)).astype(jnp.bfloat16)
            within = (
                jnp.dot(high, later, preferred_element_type=jnp.float32)
                + jnp.dot(middle, later, preferred_element_type=jnp.float32)
                + jnp.dot(low, later, preferred_element_type=jnp.float32)
            )
            sticks = jnp.exp(take_log + within)
            if step == 0:
                sticks = jnp.where(causal, sticks, 0.0)
            partial = jnp.dot(
                sticks.astype(jnp.bfloat16), values, preferred_element_type=jnp.float32
            )
            attended = attended + jnp.exp(carried) * partial
            carried = carried + within[:, :1] + keep_log[:, :1]
        out_ref[:, own] = attended.astype(out_ref.dtype)


def attend(queries, key_part, value_part, logit_part):
    tok_rows, width = queries.shape
    head_count = logit_part.shape[1]
    ring = lax.axis_size("sp")
    logit_rows = jnp.pad(jnp.transpose(logit_part), ((0, pad_rows - head_count), (0, 0)))
    packed = call(
        pack_kernel,
        "pack_blocks",
        jax.ShapeDtypeStruct((tok_rows + pad_rows, 2 * width), key_part.dtype),
        1,
        key_part,
        value_part,
        logit_rows,
    )
    blocks = [packed] + [upward(packed, "sp", step) for step in range(1, ring)]
    attended = call(
        functools.partial(attend_kernel, head_count),
        "attend",
        jax.ShapeDtypeStruct((tok_rows, width), jnp.bfloat16),
        10 * ring * tok_rows * tok_rows * width,
        queries,
        *blocks,
    )
    return attended, packed


def spread(weight):
    ring, own = lax.axis_size("sp"), lax.axis_index("sp")
    copies, copy = lax.axis_size("grp"), lax.axis_index("grp")
    rows, columns = weight.shape
    part, share = columns // ring, rows // copies
    pieces = weight.reshape(rows, ring, part).transpose(1, 0, 2)
    result = jnp.zeros((ring * rows, part), weight.dtype)
    mine = lax.dynamic_index_in_dim(pieces, own, 0, keepdims=False)
    result = lax.dynamic_update_slice(result, mine, (own * rows, 0))
    for step in range(1, ring):
        target, source = (own + step) % ring, (own - step) % ring
        piece = lax.dynamic_slice(pieces, (target, copy * share, 0), (1, share, part))[0]
        piece = shift(piece, "sp", step)
        for turn in range(copies):
            other = piece if turn == 0 else shift(piece, "grp", turn)
            place = (copy - turn) % copies
            result = lax.dynamic_update_slice(result, other, (source * rows + place * share, 0))
    return result


def tile_at(ref, rows, ring, target):
    main = ref.shape[1] // ring // lanes * lanes
    start = pl.multiple_of(ring * main + target // 2 * lanes, lanes)
    return ref[rows, pl.ds(start, lanes)].astype(jnp.float32)


def main_at(ref, rows, ring, target):
    main = ref.shape[1] // ring // lanes * lanes
    return ref[rows, pl.ds(pl.multiple_of(target * main, lanes), main)]


def halves(low, high, odd):
    lower = lax.broadcasted_iota(jnp.int32, low.shape, 1) < lanes // 2
    low = jnp.where(odd, pltpu.roll(low, lanes // 2, 1), low)
    high = jnp.where(odd, high, pltpu.roll(high, lanes // 2, 1))
    return jnp.where(lower, low, high).astype(jnp.bfloat16)


def pack_wide_kernel(ring, where_ref, gate_ref, up_ref, own_ref, *out_refs):
    own, copy = where_ref[0], where_ref[1]
    share = out_refs[0].shape[0]
    for step in range(ring):
        target = lax.rem(own + step, ring)
        out = own_ref if step == 0 else out_refs[step - 1]
        rows = slice(None) if step == 0 else pl.ds(pl.multiple_of(copy * share, share), share)
        gate, up = main_at(gate_ref, rows, ring, target), main_at(up_ref, rows, ring, target)
        main = gate.shape[1]
        out[:, :main] = gate
        out[:, main : 2 * main] = up
        out[:, 2 * main :] = halves(
            tile_at(gate_ref, rows, ring, target),
            tile_at(up_ref, rows, ring, target),
            target % 2 == 1,
        )


def pack_narrow_kernel(ring, where_ref, down_ref, *out_refs):
    own, copy = where_ref[0], where_ref[1]
    half = out_refs[0].shape[0]
    copies = down_ref.shape[0] // (2 * half)
    for step in range(1 - copies, ring):
        target = lax.rem(own + max(step, 0), ring)
        out = out_refs[step + copies - 1]
        start = (step + copies - 1) * 2 * half if step <= 0 else copy * 2 * half
        upper = pl.ds(pl.multiple_of(start, half), half)
        lower = pl.ds(pl.multiple_of(start + half, half), half)
        main = (out.shape[1] - lanes) // 2
        out[:, :main] = main_at(down_ref, upper, ring, target)
        out[:, main : 2 * main] = main_at(down_ref, lower, ring, target)
        out[:, 2 * main :] = halves(
            tile_at(down_ref, upper, ring, target),
            tile_at(down_ref, lower, ring, target),
            target % 2 == 1,
        )


def exchange(pieces):
    copies = lax.axis_size("grp")
    arrived = []
    for step, piece in enumerate(pieces, 1):
        piece = shift(piece, "sp", step)
        arrived.append([piece] + [shift(piece, "grp", turn) for turn in range(1, copies)])
    return arrived


def wide_kernel(ring, copies, where_ref, rows_ref, *refs):
    own_ref, pieces, (low_ref, high_ref), weight = refs[0], refs[1:-3], refs[-3:-1], refs[-1]
    own, copy = where_ref[0], where_ref[1]
    depth, share = own_ref.shape[0], pieces[0].shape[0]
    weight[pl.ds(pl.multiple_of(own * depth, depth), depth), :] = own_ref[...]
    for step in range(1, ring):
        for turn in range(copies):
            source = lax.rem(own - step + ring, ring)
            place = lax.rem(copy - turn + copies, copies)
            start = pl.multiple_of(source * depth + place * share, share)
            weight[pl.ds(start, share), :] = pieces[(step - 1) * copies + turn][...]
    main = (own_ref.shape[1] - lanes) // 2
    count = rows_ref.shape[0]
    tile = min(count, 256)

    def body(index, _):
        rows = pl.ds(pl.multiple_of(index * tile, tile), tile)
        block = rows_ref[rows, :]
        gate = jnp.dot(block, weight[:, :main], preferred_element_type=jnp.float32)
        up = jnp.dot(block, weight[:, main : 2 * main], preferred_element_type=jnp.float32)
        both = jnp.dot(block, weight[:, 2 * main :], preferred_element_type=jnp.float32)
        hidden = (gate / (1.0 + jnp.exp(-gate)) * up).astype(jnp.bfloat16)
        rest = both / (1.0 + jnp.exp(-both)) * pltpu.roll(both, lanes // 2, 1)
        lower = lax.broadcasted_iota(jnp.int32, rest.shape, 1) < lanes // 2
        rest = jnp.where(lower, rest, 0.0)
        low_ref[rows, :main] = hidden
        high_ref[rows, :main] = hidden
        low_ref[rows, main:] = rest.astype(jnp.bfloat16)
        high_ref[rows, main:] = pltpu.roll(rest, lanes // 2, 1).astype(jnp.bfloat16)
        return 0

    lax.fori_loop(0, count // tile, body, 0)


def narrow_kernel(ring, copies, where_ref, low_ref, high_ref, *refs):
    own_refs, pieces, outs, weights = refs[:copies], refs[copies:-4], refs[-4:-2], refs[-2:]
    own, copy = where_ref[0], where_ref[1]
    half = own_refs[0].shape[0]
    main = (own_refs[0].shape[1] - lanes) // 2

    def place_piece(ref, source, place):
        start = pl.multiple_of((source * copies + place) * half, half)
        for part, weight in enumerate(weights):
            weight[pl.ds(start, half), :main] = ref[:, part * main : (part + 1) * main]
            weight[pl.ds(start, half), main:] = ref[:, 2 * main :]

    for place in range(copies):
        place_piece(own_refs[place], own, place)
    for step in range(1, ring):
        for turn in range(copies):
            source = lax.rem(own - step + ring, ring)
            place = lax.rem(copy - turn + copies, copies)
            place_piece(pieces[(step - 1) * copies + turn], source, place)
    count = outs[0].shape[0]
    for index, out in enumerate(outs):
        rows = slice(index * count, (index + 1) * count)
        for part, hidden_ref in enumerate((low_ref, high_ref)):
            units = dot_t(hidden_ref[rows, :], weights[part][...]).astype(jnp.bfloat16)
            for block in range(ring * copies):
                start = (2 * block + part) * half
                out[:, start : start + half] = units[:, block * half : (block + 1) * half]


def shards(
    query_rows,
    key_rows,
    value_rows,
    key_logit,
    residual,
    out_weight,
    mix_gain,
    ffn_gain,
    out_gain,
    gate_weight,
    up_weight,
    down_weight,
):
    ring, own = lax.axis_size("sp"), lax.axis_index("sp")
    copies, copy = lax.axis_size("grp"), lax.axis_index("grp")
    members, member = lax.axis_size("tp"), lax.axis_index("tp")
    tok_rows, width = residual.shape
    own_rows = tok_rows // members
    bits = [1 << i for i in range(members.bit_length() - 1)]
    depth, part = gate_weight.shape[0], gate_weight.shape[1] // ring
    main, share = part // lanes * lanes, depth // copies
    packs = main > 0 and 2 * (part - main) == lanes and ring % 2 == 0 and share % 32 == 0
    where = jnp.stack([own, copy]).astype(jnp.int32)

    attended, packed = attend(query_rows, key_rows, value_rows, key_logit)
    if packs:
        shape = jax.ShapeDtypeStruct
        gate_in, up_in, _ = lax.optimization_barrier((gate_weight, up_weight, packed))
        wide_own, *wide = call(
            functools.partial(pack_wide_kernel, ring),
            "pack_wide",
            [shape((depth, 2 * part), jnp.bfloat16)]
            + [shape((share, 2 * part), jnp.bfloat16)] * (ring - 1),
            1,
            where,
            gate_in,
            up_in,
            scalars=1,
        )
        wide = [piece for group in exchange(wide) for piece in group]

    head_part = jnp.dot(attended, out_weight, preferred_element_type=jnp.float32)
    head_part = head_part.astype(jnp.bfloat16).reshape(members, own_rows, width)
    mixed = jnp.zeros((own_rows, width), jnp.float32)
    for step in range(members):
        piece = lax.dynamic_index_in_dim(head_part, member ^ step, 0, keepdims=False)
        piece = piece if step == 0 else swap(piece, "tp", step)
        mixed = mixed + piece.astype(jnp.float32)
    mixed = mixed.astype(jnp.bfloat16)
    own_residual = lax.dynamic_slice_in_dim(residual, member * own_rows, own_rows, 0)
    middle = (
        own_residual.astype(jnp.float32) + mix_gain * normalize(mixed.astype(jnp.float32))
    ).astype(jnp.bfloat16)
    normed = (ffn_gain * normalize(middle.astype(jnp.float32))).astype(jnp.bfloat16)

    gathered = jnp.stack(
        [normed if step == 0 else shift(normed, "sp", step) for step in range(ring)]
    )[None]
    for bit in reversed(bits):
        gathered = jnp.concatenate([gathered, swap(gathered, "tp", bit)], axis=0)
    gathered = gathered.reshape(members * ring * own_rows, width)
    all_rows = gathered.shape[0]

    if packs:
        down_in, _ = lax.optimization_barrier((down_weight, normed))
        narrow = call(
            functools.partial(pack_narrow_kernel, ring),
            "pack_narrow",
            [shape((share // 2, 2 * part), jnp.bfloat16)] * (ring - 1 + copies),
            1,
            where,
            down_in,
            scalars=1,
        )
        narrow_own, narrow = narrow[:copies], narrow[copies:]
        narrow = [piece for group in exchange(narrow) for piece in group]
        hidden = call(
            functools.partial(wide_kernel, ring, copies),
            "wide",
            [shape((all_rows, main + lanes), jnp.bfloat16)] * 2,
            4 * all_rows * width * part,
            where,
            gathered,
            wide_own,
            *wide,
            scalars=1,
            scratch=[pltpu.VMEM((width, 2 * part), jnp.bfloat16)],
            limit=40 << 20,
        )
        kept, sent = call(
            functools.partial(narrow_kernel, ring, copies),
            "narrow",
            [shape((all_rows // 2, width), jnp.bfloat16)] * 2,
            2 * all_rows * width * part,
            where,
            *hidden,
            *narrow_own,
            *narrow,
            scalars=1,
            scratch=[pltpu.VMEM((width // 2, main + lanes), jnp.bfloat16)] * 2,
            limit=40 << 20,
        )
        kept = kept.reshape(members // 2, ring, own_rows, width)
        sent = sent.reshape(members // 2, ring, own_rows, width)
    else:
        gate_full, up_full, down_full = spread(gate_weight), spread(up_weight), spread(down_weight)
        gate_act = jnp.dot(gathered, gate_full, preferred_element_type=jnp.float32)
        up_act = jnp.dot(gathered, up_full, preferred_element_type=jnp.float32)
        hidden = (jax.nn.silu(gate_act) * up_act).astype(jnp.bfloat16)
        unit_part = lax.dot_general(
            hidden, down_full, (((1,), (1,)), ((), ())), preferred_element_type=jnp.float32
        ).astype(jnp.bfloat16)
        unit_part = unit_part.reshape(members, ring, own_rows, width)
        kept, sent = jnp.split(unit_part, 2, axis=0)
    for bit in bits:
        unit_part = (
            kept.astype(jnp.float32) + swap(sent, "tp", bit).astype(jnp.float32)
        ).astype(jnp.bfloat16)
        if unit_part.shape[0] > 1:
            kept, sent = jnp.split(unit_part, 2, axis=0)
    unit_part = unit_part[0]
    ffn_out = unit_part[0].astype(jnp.float32)
    for step in range(1, ring):
        ffn_out = ffn_out + shift(unit_part[step], "sp", -step).astype(jnp.float32)
    ffn_out = ffn_out.astype(jnp.bfloat16)
    layer_out = (
        middle.astype(jnp.float32) + out_gain * normalize(ffn_out.astype(jnp.float32))
    ).astype(jnp.bfloat16)
    block = layer_out[None]
    for bit in reversed(bits):
        block = jnp.concatenate([block, swap(block, "tp", bit)], axis=0)
    result = jnp.zeros((tok_rows, width), jnp.bfloat16)
    order = [0]
    for bit in reversed(bits):
        order = order + [o ^ bit for o in order]
    for slot, offset in enumerate(order):
        result = lax.dynamic_update_slice(
            result, block[slot], ((member ^ offset) * own_rows, 0)
        )
    return result


def solution(mesh):
    placed = (
        P(("grp", "sp"), "tp"),
        P(("grp", "sp"), "tp"),
        P(("grp", "sp"), "tp"),
        P(("grp", "sp"), "tp"),
        P(("grp", "sp"), None),
        P("tp", None),
        P(),
        P(),
        P(),
        P("sp", "tp"),
        P("sp", "tp"),
        P("sp", "tp"),
    )
    return jax.shard_map(
        shards, mesh=mesh, in_specs=placed, out_specs=P(("grp", "sp"), None), check_vma=False
    )
```

```python
import functools

import jax
import jax.numpy as jnp
from jax import lax
from jax.experimental import pallas as pl
from jax.experimental.pallas import tpu as pltpu
from jax.sharding import PartitionSpec as P


epsilon = 1e-06
lanes = 128
pad_rows = 16


def normalize(payload_table):
    return payload_table * lax.rsqrt(
        jnp.mean(payload_table * payload_table, axis=-1, keepdims=True) + epsilon
    )


def shift(rows, axis, step):
    count = lax.axis_size(axis)
    return lax.ppermute(rows, axis, [(i, (i + step) % count) for i in range(count)])


def upward(rows, axis, step):
    count = lax.axis_size(axis)
    return lax.ppermute(rows, axis, [(i, i + step) for i in range(count - step)])


def swap(rows, axis, bit):
    count = lax.axis_size(axis)
    return lax.ppermute(rows, axis, [(i, i ^ bit) for i in range(count)])


def call(kernel, outs, flops, *args, scalars=0, scratch=(), limit=None):
    specs = [pl.BlockSpec(memory_space=pltpu.SMEM)] * scalars
    specs += [pl.BlockSpec(memory_space=pltpu.VMEM)] * (len(args) - scalars)
    single = not isinstance(outs, list)
    out_list = [outs] if single else outs
    moved = sum(a.size * a.dtype.itemsize for a in (*args, *out_list))
    out_specs = [pl.BlockSpec(memory_space=pltpu.VMEM)] * len(out_list)
    return pl.pallas_call(
        kernel,
        out_shape=outs,
        in_specs=specs,
        out_specs=out_specs[0] if single else out_specs,
        scratch_shapes=list(scratch),
        compiler_params=pltpu.CompilerParams(vmem_limit_bytes=limit),
        cost_estimate=pl.CostEstimate(flops=flops, bytes_accessed=moved, transcendentals=0),
    )(*args)


def dot_t(a, b):
    return lax.dot_general(a, b, (((1,), (1,)), ((), ())), preferred_element_type=jnp.float32)


def pack_kernel(key_ref, value_ref, logit_ref, out_ref):
    tok_rows, width = key_ref.shape
    out_ref[:tok_rows, :width] = key_ref[...]
    out_ref[:tok_rows, width:] = value_ref[...]
    out_ref[tok_rows:, :tok_rows] = logit_ref[...]
    out_ref[tok_rows:, tok_rows:] = jnp.zeros((pad_rows, 2 * width - tok_rows), out_ref.dtype)


def attend_kernel(head_count, query_ref, *refs):
    blocks, out_ref = refs[:-1], refs[-1]
    tok_rows, width = query_ref.shape
    head_width = width // head_count
    row = lax.broadcasted_iota(jnp.int32, (tok_rows, tok_rows), 0)
    column = lax.broadcasted_iota(jnp.int32, (tok_rows, tok_rows), 1)
    causal = row > column
    later = causal.astype(jnp.float32).astype(jnp.bfloat16)
    for head in range(head_count):
        own = slice(head * head_width, (head + 1) * head_width)
        queries = query_ref[:, own]
        attended = jnp.zeros((tok_rows, head_width), jnp.float32)
        carried = jnp.zeros((tok_rows, 1), jnp.float32)
        for step, block in enumerate(blocks):
            keys = block[:tok_rows, own]
            values = block[:tok_rows, width + head * head_width : width + (head + 1) * head_width]
            logit = block[tok_rows:, :tok_rows].astype(jnp.float32)[head : head + 1]
            scores = dot_t(queries, keys) * head_width ** (-0.5) + logit
            tail = jnp.log(1.0 + jnp.exp(-jnp.abs(scores)))
            keep_log = -jnp.maximum(scores, 0.0) - tail
            take_log = jnp.minimum(scores, 0.0) - tail
            if step == 0:
                keep_log = jnp.where(causal, keep_log, 0.0)
            high = keep_log.astype(jnp.bfloat16)
            rest = keep_log - high.astype(jnp.float32)
            middle = rest.astype(jnp.bfloat16)
            low = (rest - middle.astype(jnp.float32)).astype(jnp.bfloat16)
            within = (
                jnp.dot(high, later, preferred_element_type=jnp.float32)
                + jnp.dot(middle, later, preferred_element_type=jnp.float32)
                + jnp.dot(low, later, preferred_element_type=jnp.float32)
            )
            sticks = jnp.exp(take_log + within)
            if step == 0:
                sticks = jnp.where(causal, sticks, 0.0)
            partial = jnp.dot(
                sticks.astype(jnp.bfloat16), values, preferred_element_type=jnp.float32
            )
            attended = attended + jnp.exp(carried) * partial
            carried = carried + within[:, :1] + keep_log[:, :1]
        out_ref[:, own] = attended.astype(out_ref.dtype)


def attend(queries, key_part, value_part, logit_part):
    tok_rows, width = queries.shape
    head_count = logit_part.shape[1]
    ring = lax.axis_size("sp")
    logit_rows = jnp.pad(jnp.transpose(logit_part), ((0, pad_rows - head_count), (0, 0)))
    packed = call(
        pack_kernel,
        jax.ShapeDtypeStruct((tok_rows + pad_rows, 2 * width), key_part.dtype),
        1,
        key_part,
        value_part,
        logit_rows,
    )
    blocks = [packed] + [upward(packed, "sp", step) for step in range(1, ring)]
    attended = call(
        functools.partial(attend_kernel, head_count),
        jax.ShapeDtypeStruct((tok_rows, width), jnp.bfloat16),
        10 * ring * tok_rows * tok_rows * width,
        queries,
        *blocks,
    )
    return attended, packed


def spread(weight):
    ring, own = lax.axis_size("sp"), lax.axis_index("sp")
    copies, copy = lax.axis_size("grp"), lax.axis_index("grp")
    rows, columns = weight.shape
    part, share = columns // ring, rows // copies
    pieces = weight.reshape(rows, ring, part).transpose(1, 0, 2)
    result = jnp.zeros((ring * rows, part), weight.dtype)
    mine = lax.dynamic_index_in_dim(pieces, own, 0, keepdims=False)
    result = lax.dynamic_update_slice(result, mine, (own * rows, 0))
    for step in range(1, ring):
        target, source = (own + step) % ring, (own - step) % ring
        piece = lax.dynamic_slice(pieces, (target, copy * share, 0), (1, share, part))[0]
        piece = shift(piece, "sp", step)
        for turn in range(copies):
            other = piece if turn == 0 else shift(piece, "grp", turn)
            place = (copy - turn) % copies
            result = lax.dynamic_update_slice(result, other, (source * rows + place * share, 0))
    return result


def tile_at(ref, rows, ring, target):
    main = ref.shape[1] // ring // lanes * lanes
    start = pl.multiple_of(ring * main + target // 2 * lanes, lanes)
    return ref[rows, pl.ds(start, lanes)].astype(jnp.float32)


def main_at(ref, rows, ring, target):
    main = ref.shape[1] // ring // lanes * lanes
    return ref[rows, pl.ds(pl.multiple_of(target * main, lanes), main)]


def halves(low, high, odd):
    lower = lax.broadcasted_iota(jnp.int32, low.shape, 1) < lanes // 2
    low = jnp.where(odd, pltpu.roll(low, lanes // 2, 1), low)
    high = jnp.where(odd, high, pltpu.roll(high, lanes // 2, 1))
    return jnp.where(lower, low, high).astype(jnp.bfloat16)


def pack_wide_kernel(ring, where_ref, gate_ref, up_ref, own_ref, *out_refs):
    own, copy = where_ref[0], where_ref[1]
    share = out_refs[0].shape[0]
    for step in range(ring):
        target = lax.rem(own + step, ring)
        out = own_ref if step == 0 else out_refs[step - 1]
        rows = slice(None) if step == 0 else pl.ds(pl.multiple_of(copy * share, share), share)
        gate, up = main_at(gate_ref, rows, ring, target), main_at(up_ref, rows, ring, target)
        main = gate.shape[1]
        out[:, :main] = gate
        out[:, main : 2 * main] = up
        out[:, 2 * main :] = halves(
            tile_at(gate_ref, rows, ring, target),
            tile_at(up_ref, rows, ring, target),
            target % 2 == 1,
        )


def pack_narrow_kernel(ring, where_ref, down_ref, *out_refs):
    own, copy = where_ref[0], where_ref[1]
    half = out_refs[0].shape[0]
    copies = down_ref.shape[0] // (2 * half)
    for step in range(1 - copies, ring):
        target = lax.rem(own + max(step, 0), ring)
        out = out_refs[step + copies - 1]
        start = (step + copies - 1) * 2 * half if step <= 0 else copy * 2 * half
        upper = pl.ds(pl.multiple_of(start, half), half)
        lower = pl.ds(pl.multiple_of(start + half, half), half)
        main = (out.shape[1] - lanes) // 2
        out[:, :main] = main_at(down_ref, upper, ring, target)
        out[:, main : 2 * main] = main_at(down_ref, lower, ring, target)
        out[:, 2 * main :] = halves(
            tile_at(down_ref, upper, ring, target),
            tile_at(down_ref, lower, ring, target),
            target % 2 == 1,
        )


def exchange(pieces):
    copies = lax.axis_size("grp")
    arrived = []
    for step, piece in enumerate(pieces, 1):
        piece = shift(piece, "sp", step)
        arrived.append([piece] + [shift(piece, "grp", turn) for turn in range(1, copies)])
    return arrived


def wide_kernel(ring, copies, block_count, where_ref, *refs):
    blocks, refs = refs[:block_count], refs[block_count:]
    own_ref, pieces, (low_ref, high_ref), scratch = refs[0], refs[1:-4], refs[-4:-2], refs[-2:]
    weight, rows_ref = scratch
    own, copy = where_ref[0], where_ref[1]
    block_rows = blocks[0].shape[0]
    for index, block in enumerate(blocks):
        rows_ref[index * block_rows : (index + 1) * block_rows, :] = block[...]
    depth, share = own_ref.shape[0], pieces[0].shape[0]
    weight[pl.ds(pl.multiple_of(own * depth, depth), depth), :] = own_ref[...]
    for step in range(1, ring):
        for turn in range(copies):
            source = lax.rem(own - step + ring, ring)
            place = lax.rem(copy - turn + copies, copies)
            start = pl.multiple_of(source * depth + place * share, share)
            weight[pl.ds(start, share), :] = pieces[(step - 1) * copies + turn][...]
    main = (own_ref.shape[1] - lanes) // 2
    count = rows_ref.shape[0]
    tile = min(count, 256)

    def body(index, _):
        rows = pl.ds(pl.multiple_of(index * tile, tile), tile)
        block = rows_ref[rows, :]
        gate = jnp.dot(block, weight[:, :main], preferred_element_type=jnp.float32)
        up = jnp.dot(block, weight[:, main : 2 * main], preferred_element_type=jnp.float32)
        both = jnp.dot(block, weight[:, 2 * main :], preferred_element_type=jnp.float32)
        hidden = (gate / (1.0 + jnp.exp(-gate)) * up).astype(jnp.bfloat16)
        rest = both / (1.0 + jnp.exp(-both)) * pltpu.roll(both, lanes // 2, 1)
        lower = lax.broadcasted_iota(jnp.int32, rest.shape, 1) < lanes // 2
        rest = jnp.where(lower, rest, 0.0)
        low_ref[rows, :main] = hidden
        high_ref[rows, :main] = hidden
        low_ref[rows, main:] = rest.astype(jnp.bfloat16)
        high_ref[rows, main:] = pltpu.roll(rest, lanes // 2, 1).astype(jnp.bfloat16)
        return 0

    lax.fori_loop(0, count // tile, body, 0)


def narrow_kernel(ring, copies, where_ref, low_ref, high_ref, *refs):
    own_refs, pieces, outs, weights = refs[:copies], refs[copies:-4], refs[-4:-2], refs[-2:]
    own, copy = where_ref[0], where_ref[1]
    half = own_refs[0].shape[0]
    main = (own_refs[0].shape[1] - lanes) // 2

    def place_piece(ref, source, place):
        start = pl.multiple_of((source * copies + place) * half, half)
        for part, weight in enumerate(weights):
            weight[pl.ds(start, half), :main] = ref[:, part * main : (part + 1) * main]
            weight[pl.ds(start, half), main:] = ref[:, 2 * main :]

    for place in range(copies):
        place_piece(own_refs[place], own, place)
    for step in range(1, ring):
        for turn in range(copies):
            source = lax.rem(own - step + ring, ring)
            place = lax.rem(copy - turn + copies, copies)
            place_piece(pieces[(step - 1) * copies + turn], source, place)
    count = outs[0].shape[0]
    for index, out in enumerate(outs):
        rows = slice(index * count, (index + 1) * count)
        for part, hidden_ref in enumerate((low_ref, high_ref)):
            units = dot_t(hidden_ref[rows, :], weights[part][...]).astype(jnp.bfloat16)
            for block in range(ring * copies):
                start = (2 * block + part) * half
                out[:, start : start + half] = units[:, block * half : (block + 1) * half]


def join_kernel(member_ref, *refs):
    parts, out_ref = refs[:-1], refs[-1]
    rows = parts[0].shape[0]
    for offset, part in enumerate(parts):
        start = pl.multiple_of((member_ref[0] ^ offset) * rows, rows)
        out_ref[pl.ds(start, rows), :] = part[...]


def shards(
    query_rows,
    key_rows,
    value_rows,
    key_logit,
    residual,
    out_weight,
    mix_gain,
    ffn_gain,
    out_gain,
    gate_weight,
    up_weight,
    down_weight,
):
    ring, own = lax.axis_size("sp"), lax.axis_index("sp")
    copies, copy = lax.axis_size("grp"), lax.axis_index("grp")
    members, member = lax.axis_size("tp"), lax.axis_index("tp")
    tok_rows, width = residual.shape
    own_rows = tok_rows // members
    bits = [1 << i for i in range(members.bit_length() - 1)]
    depth, part = gate_weight.shape[0], gate_weight.shape[1] // ring
    main, share = part // lanes * lanes, depth // copies
    packs = main > 0 and 2 * (part - main) == lanes and ring % 2 == 0 and share % 32 == 0
    where = jnp.stack([own, copy]).astype(jnp.int32)

    attended, packed = attend(query_rows, key_rows, value_rows, key_logit)
    if packs:
        shape = jax.ShapeDtypeStruct
        gate_in, up_in, _ = lax.optimization_barrier((gate_weight, up_weight, packed))
        wide_own, *wide = call(
            functools.partial(pack_wide_kernel, ring),
            [shape((depth, 2 * part), jnp.bfloat16)]
            + [shape((share, 2 * part), jnp.bfloat16)] * (ring - 1),
            1,
            where,
            gate_in,
            up_in,
            scalars=1,
        )
        wide = [piece for group in exchange(wide) for piece in group]

    head_part = jnp.dot(attended, out_weight, preferred_element_type=jnp.float32)
    head_part = head_part.astype(jnp.bfloat16).reshape(members, own_rows, width)
    mixed = jnp.zeros((own_rows, width), jnp.float32)
    for step in range(members):
        piece = lax.dynamic_index_in_dim(head_part, member ^ step, 0, keepdims=False)
        piece = piece if step == 0 else swap(piece, "tp", step)
        mixed = mixed + piece.astype(jnp.float32)
    mixed = mixed.astype(jnp.bfloat16)
    own_residual = lax.dynamic_slice_in_dim(residual, member * own_rows, own_rows, 0)
    middle = (
        own_residual.astype(jnp.float32) + mix_gain * normalize(mixed.astype(jnp.float32))
    ).astype(jnp.bfloat16)
    normed = (ffn_gain * normalize(middle.astype(jnp.float32))).astype(jnp.bfloat16)

    if packs:
        narrow = call(
            functools.partial(pack_narrow_kernel, ring),
            [shape((share // 2, 2 * part), jnp.bfloat16)] * (ring - 1 + copies),
            1,
            where,
            down_weight,
            scalars=1,
        )
        narrow_own, narrow = narrow[:copies], narrow[copies:]
        narrow = [piece for group in exchange(narrow) for piece in group]

        blocks = {(0, 0): normed}
        for step in range(1, ring):
            blocks[0, step] = shift(normed, "sp", step)
        for bit in reversed(bits):
            for (offset, step), block in list(blocks.items()):
                blocks[offset ^ bit, step] = swap(block, "tp", bit)
        order = [(2 * p + half, k) for half in range(2) for p in range(members // 2) for k in range(ring)]
        all_rows = len(order) * own_rows
        hidden = call(
            functools.partial(wide_kernel, ring, copies, len(order)),
            [shape((all_rows, main + lanes), jnp.bfloat16)] * 2,
            4 * all_rows * width * part,
            where,
            *[blocks[key] for key in order],
            wide_own,
            *wide,
            scalars=1,
            scratch=[
                pltpu.VMEM((width, 2 * part), jnp.bfloat16),
                pltpu.VMEM((all_rows, width), jnp.bfloat16),
            ],
            limit=40 << 20,
        )
        kept, sent = call(
            functools.partial(narrow_kernel, ring, copies),
            [shape((all_rows // 2, width), jnp.bfloat16)] * 2,
            2 * all_rows * width * part,
            where,
            *hidden,
            *narrow_own,
            *narrow,
            scalars=1,
            scratch=[pltpu.VMEM((width // 2, main + lanes), jnp.bfloat16)] * 2,
            limit=40 << 20,
        )
        arrived = swap(sent, "tp", 1)
        kept = kept.reshape(members // 2, ring, own_rows, width)
        arrived = arrived.reshape(members // 2, ring, own_rows, width)
        ffn_out = jnp.zeros((own_rows, width), jnp.float32)
        for step in [*range(1, ring), 0]:
            units = kept[:, step].astype(jnp.float32) + arrived[:, step].astype(jnp.float32)
            for bit in bits[1:]:
                moved = swap(units[1::2].astype(jnp.bfloat16), "tp", bit)
                units = units[0::2] + moved.astype(jnp.float32)
            units = units[0]
            if step:
                units = shift(units.astype(jnp.bfloat16), "sp", -step).astype(jnp.float32)
            ffn_out = ffn_out + units
    else:
        gathered = jnp.stack(
            [normed if step == 0 else shift(normed, "sp", step) for step in range(ring)]
        )[None]
        for bit in reversed(bits):
            gathered = jnp.concatenate([gathered, swap(gathered, "tp", bit)], axis=0)
        gathered = gathered.reshape(members * ring * own_rows, width)
        gate_full, up_full, down_full = spread(gate_weight), spread(up_weight), spread(down_weight)
        gate_act = jnp.dot(gathered, gate_full, preferred_element_type=jnp.float32)
        up_act = jnp.dot(gathered, up_full, preferred_element_type=jnp.float32)
        hidden = (jax.nn.silu(gate_act) * up_act).astype(jnp.bfloat16)
        unit_part = lax.dot_general(
            hidden, down_full, (((1,), (1,)), ((), ())), preferred_element_type=jnp.float32
        ).astype(jnp.bfloat16)
        unit_part = unit_part.reshape(members, ring, own_rows, width)
        for bit in bits:
            kept, sent = jnp.split(unit_part, 2, axis=0)
            unit_part = (
                kept.astype(jnp.float32) + swap(sent, "tp", bit).astype(jnp.float32)
            ).astype(jnp.bfloat16)
        ffn_out = unit_part[0, 0].astype(jnp.float32)
        for step in range(1, ring):
            ffn_out = ffn_out + shift(unit_part[0, step], "sp", -step).astype(jnp.float32)
    ffn_out = ffn_out.astype(jnp.bfloat16)
    layer_out = (
        middle.astype(jnp.float32) + out_gain * normalize(ffn_out.astype(jnp.float32))
    ).astype(jnp.bfloat16)
    parts = {0: layer_out}
    for bit in reversed(bits):
        for offset, rows in list(parts.items()):
            parts[offset ^ bit] = swap(rows, "tp", bit)
    return call(
        join_kernel,
        jax.ShapeDtypeStruct((tok_rows, width), jnp.bfloat16),
        1,
        member[None].astype(jnp.int32),
        *[parts[offset] for offset in range(members)],
        scalars=1,
    )


def solution(mesh):
    placed = (
        P(("grp", "sp"), "tp"),
        P(("grp", "sp"), "tp"),
        P(("grp", "sp"), "tp"),
        P(("grp", "sp"), "tp"),
        P(("grp", "sp"), None),
        P("tp", None),
        P(),
        P(),
        P(),
        P("sp", "tp"),
        P("sp", "tp"),
        P("sp", "tp"),
    )
    return jax.shard_map(
        shards, mesh=mesh, in_specs=placed, out_specs=P(("grp", "sp"), None), check_vma=False
    )
```

```python
import functools

import jax
import jax.numpy as jnp
from jax import lax
from jax.experimental import pallas as pl
from jax.experimental.pallas import tpu as pltpu
from jax.sharding import PartitionSpec as P


epsilon = 1e-06
lanes = 128
pad_rows = 16


def normalize(payload_table):
    return payload_table * lax.rsqrt(
        jnp.mean(payload_table * payload_table, axis=-1, keepdims=True) + epsilon
    )


def shift(rows, axis, step):
    count = lax.axis_size(axis)
    return lax.ppermute(rows, axis, [(i, (i + step) % count) for i in range(count)])


def upward(rows, axis, step):
    count = lax.axis_size(axis)
    return lax.ppermute(rows, axis, [(i, i + step) for i in range(count - step)])


def swap(rows, axis, bit):
    count = lax.axis_size(axis)
    return lax.ppermute(rows, axis, [(i, i ^ bit) for i in range(count)])


def call(kernel, outs, flops, *args, scratch=(), limit=None):
    specs = [pl.BlockSpec(memory_space=pltpu.VMEM)] * len(args)
    single = not isinstance(outs, list)
    out_list = [outs] if single else outs
    moved = sum(a.size * a.dtype.itemsize for a in (*args, *out_list))
    out_specs = [pl.BlockSpec(memory_space=pltpu.VMEM)] * len(out_list)
    return pl.pallas_call(
        kernel,
        out_shape=outs,
        in_specs=specs,
        out_specs=out_specs[0] if single else out_specs,
        scratch_shapes=list(scratch),
        compiler_params=pltpu.CompilerParams(vmem_limit_bytes=limit),
        cost_estimate=pl.CostEstimate(flops=flops, bytes_accessed=moved, transcendentals=0),
    )(*args)


def dot_t(a, b):
    return lax.dot_general(a, b, (((1,), (1,)), ((), ())), preferred_element_type=jnp.float32)


def pack_kernel(key_ref, value_ref, logit_ref, out_ref):
    tok_rows, width = key_ref.shape
    out_ref[:tok_rows, :width] = key_ref[...]
    out_ref[:tok_rows, width:] = value_ref[...]
    head_count = logit_ref.shape[1]
    row = lax.broadcasted_iota(jnp.int32, (pad_rows, head_count), 0)
    column = lax.broadcasted_iota(jnp.int32, (pad_rows, head_count), 1)
    pick = (row == column).astype(jnp.float32).astype(jnp.bfloat16)
    out_ref[tok_rows:, :tok_rows] = dot_t(pick, logit_ref[...]).astype(out_ref.dtype)
    out_ref[tok_rows:, tok_rows:] = jnp.zeros((pad_rows, 2 * width - tok_rows), out_ref.dtype)


def attend_kernel(head_count, query_ref, *refs):
    blocks, out_ref = refs[:-1], refs[-1]
    tok_rows, width = query_ref.shape
    head_width = width // head_count
    row = lax.broadcasted_iota(jnp.int32, (tok_rows, tok_rows), 0)
    column = lax.broadcasted_iota(jnp.int32, (tok_rows, tok_rows), 1)
    causal = row > column
    later = causal.astype(jnp.float32).astype(jnp.bfloat16)
    for head in range(head_count):
        own = slice(head * head_width, (head + 1) * head_width)
        queries = query_ref[:, own]
        attended = jnp.zeros((tok_rows, head_width), jnp.float32)
        carried = jnp.zeros((tok_rows, 1), jnp.float32)
        for step, block in enumerate(blocks):
            keys = block[:tok_rows, own]
            values = block[:tok_rows, width + head * head_width : width + (head + 1) * head_width]
            logit = block[tok_rows:, :tok_rows].astype(jnp.float32)[head : head + 1]
            scores = dot_t(queries, keys) * head_width ** (-0.5) + logit
            tail = jnp.log(1.0 + jnp.exp(-jnp.abs(scores)))
            keep_log = -jnp.maximum(scores, 0.0) - tail
            take_log = jnp.minimum(scores, 0.0) - tail
            if step == 0:
                keep_log = jnp.where(causal, keep_log, 0.0)
            high = keep_log.astype(jnp.bfloat16)
            rest = keep_log - high.astype(jnp.float32)
            middle = rest.astype(jnp.bfloat16)
            low = (rest - middle.astype(jnp.float32)).astype(jnp.bfloat16)
            within = (
                jnp.dot(high, later, preferred_element_type=jnp.float32)
                + jnp.dot(middle, later, preferred_element_type=jnp.float32)
                + jnp.dot(low, later, preferred_element_type=jnp.float32)
            )
            sticks = jnp.exp(take_log + within)
            if step == 0:
                sticks = jnp.where(causal, sticks, 0.0)
            partial = jnp.dot(
                sticks.astype(jnp.bfloat16), values, preferred_element_type=jnp.float32
            )
            attended = attended + jnp.exp(carried) * partial
            carried = carried + within[:, :1] + keep_log[:, :1]
        out_ref[:, own] = attended.astype(out_ref.dtype)


def attend(queries, key_part, value_part, logit_part):
    tok_rows, width = queries.shape
    head_count = logit_part.shape[1]
    ring = lax.axis_size("sp")
    packed = call(
        pack_kernel,
        jax.ShapeDtypeStruct((tok_rows + pad_rows, 2 * width), key_part.dtype),
        1,
        key_part,
        value_part,
        logit_part,
    )
    blocks = [packed] + [upward(packed, "sp", step) for step in range(1, ring)]
    attended = call(
        functools.partial(attend_kernel, head_count),
        jax.ShapeDtypeStruct((tok_rows, width), jnp.bfloat16),
        10 * ring * tok_rows * tok_rows * width,
        queries,
        *blocks,
    )
    return attended, packed


def spread(weight):
    ring, own = lax.axis_size("sp"), lax.axis_index("sp")
    copies, copy = lax.axis_size("grp"), lax.axis_index("grp")
    rows, columns = weight.shape
    part, share = columns // ring, rows // copies
    pieces = weight.reshape(rows, ring, part).transpose(1, 0, 2)
    result = jnp.zeros((ring * rows, part), weight.dtype)
    mine = lax.dynamic_index_in_dim(pieces, own, 0, keepdims=False)
    result = lax.dynamic_update_slice(result, mine, (own * rows, 0))
    for step in range(1, ring):
        target, source = (own + step) % ring, (own - step) % ring
        piece = lax.dynamic_slice(pieces, (target, copy * share, 0), (1, share, part))[0]
        piece = shift(piece, "sp", step)
        for turn in range(copies):
            other = piece if turn == 0 else shift(piece, "grp", turn)
            place = (copy - turn) % copies
            result = lax.dynamic_update_slice(result, other, (source * rows + place * share, 0))
    return result


def tile_at(ref, rows, ring, target):
    main = ref.shape[1] // ring // lanes * lanes
    start = pl.multiple_of(ring * main + target // 2 * lanes, lanes)
    return ref[rows, pl.ds(start, lanes)].astype(jnp.float32)


def main_at(ref, rows, ring, target):
    main = ref.shape[1] // ring // lanes * lanes
    return ref[rows, pl.ds(pl.multiple_of(target * main, lanes), main)]


def halves(low, high, odd):
    lower = lax.broadcasted_iota(jnp.int32, low.shape, 1) < lanes // 2
    low = jnp.where(odd, pltpu.roll(low, lanes // 2, 1), low)
    high = jnp.where(odd, high, pltpu.roll(high, lanes // 2, 1))
    return jnp.where(lower, low, high).astype(jnp.bfloat16)


def pack_wide(out, gate_ref, up_ref, rows, ring, target):
    gate, up = main_at(gate_ref, rows, ring, target), main_at(up_ref, rows, ring, target)
    count, main = gate.shape
    out[:count, :main] = gate
    out[:count, main : 2 * main] = up
    out[:count, 2 * main :] = halves(
        tile_at(gate_ref, rows, ring, target),
        tile_at(up_ref, rows, ring, target),
        target % 2 == 1,
    )


def pack_narrow(out, place, down_ref, start, half, ring, target):
    upper = pl.ds(pl.multiple_of(start, half), half)
    lower = pl.ds(pl.multiple_of(start + half, half), half)
    main = (out.shape[1] - lanes) // 2
    rows = slice(place, place + half)
    out[rows, :main] = main_at(down_ref, upper, ring, target)
    out[rows, main : 2 * main] = main_at(down_ref, lower, ring, target)
    out[rows, 2 * main :] = halves(
        tile_at(down_ref, upper, ring, target),
        tile_at(down_ref, lower, ring, target),
        target % 2 == 1,
    )


def pack_outer_kernel(ring, steps, gate_ref, up_ref, down_ref, *out_refs):
    own, copy = lax.axis_index("sp"), lax.axis_index("grp")
    for step, out in zip(steps, out_refs):
        share = out.shape[0] // 3 * 2
        target = lax.rem(own + step, ring)
        start = pl.multiple_of(copy * share, share)
        pack_wide(out, gate_ref, up_ref, pl.ds(start, share), ring, target)
        pack_narrow(out, share, down_ref, start, share // 2, ring, target)


def pack_middle_kernel(ring, step, gate_ref, up_ref, down_ref, wide_ref, narrow_ref):
    own, copy = lax.axis_index("sp"), lax.axis_index("grp")
    share = wide_ref.shape[0]
    target = lax.rem(own + step, ring)
    start = pl.multiple_of(copy * share, share)
    pack_wide(wide_ref, gate_ref, up_ref, pl.ds(start, share), ring, target)
    pack_narrow(narrow_ref, 0, down_ref, start, share // 2, ring, target)


def pack_own_kernel(ring, gate_ref, up_ref, down_ref, wide_ref, narrow_ref):
    own = lax.axis_index("sp")
    share = wide_ref.shape[0] // lax.axis_size("grp")
    pack_wide(wide_ref, gate_ref, up_ref, slice(None), ring, own)
    for copy in range(lax.axis_size("grp")):
        place = copy * share // 2
        pack_narrow(narrow_ref, place, down_ref, copy * share, share // 2, ring, own)


def exchange(piece, step):
    piece = shift(piece, "sp", step)
    turns = range(1, lax.axis_size("grp"))
    return [piece] + [shift(piece, "grp", turn) for turn in turns]


def wide_kernel(ring, copies, block_count, *refs):
    blocks, refs = refs[:block_count], refs[block_count:]
    own_ref, pieces, (low_ref, high_ref), scratch = refs[0], refs[1:-4], refs[-4:-2], refs[-2:]
    weight, rows_ref = scratch
    own, copy = lax.axis_index("sp"), lax.axis_index("grp")
    block_rows = blocks[0].shape[0]
    for index, block in enumerate(blocks):
        rows_ref[index * block_rows : (index + 1) * block_rows, :] = block[...]
    depth, share = own_ref.shape[0], own_ref.shape[0] // copies
    weight[pl.ds(pl.multiple_of(own * depth, depth), depth), :] = own_ref[...]
    for step in range(1, ring):
        for turn in range(copies):
            source = lax.rem(own - step + ring, ring)
            place = lax.rem(copy - turn + copies, copies)
            start = pl.multiple_of(source * depth + place * share, share)
            weight[pl.ds(start, share), :] = pieces[(step - 1) * copies + turn][:share]
    main = (own_ref.shape[1] - lanes) // 2
    count = rows_ref.shape[0]
    tile = min(count, 256)

    def body(index, _):
        rows = pl.ds(pl.multiple_of(index * tile, tile), tile)
        block = rows_ref[rows, :]
        gate = jnp.dot(block, weight[:, :main], preferred_element_type=jnp.float32)
        up = jnp.dot(block, weight[:, main : 2 * main], preferred_element_type=jnp.float32)
        both = jnp.dot(block, weight[:, 2 * main :], preferred_element_type=jnp.float32)
        hidden = (gate / (1.0 + jnp.exp(-gate)) * up).astype(jnp.bfloat16)
        rest = both / (1.0 + jnp.exp(-both)) * pltpu.roll(both, lanes // 2, 1)
        lower = lax.broadcasted_iota(jnp.int32, rest.shape, 1) < lanes // 2
        rest = jnp.where(lower, rest, 0.0)
        low_ref[rows, :main] = hidden
        high_ref[rows, :main] = hidden
        low_ref[rows, main:] = rest.astype(jnp.bfloat16)
        high_ref[rows, main:] = pltpu.roll(rest, lanes // 2, 1).astype(jnp.bfloat16)
        return 0

    lax.fori_loop(0, count // tile, body, 0)


def narrow_kernel(ring, copies, low_ref, high_ref, own_ref, *refs):
    pieces, weights = refs[: copies * (ring - 1)], refs[-2:]
    outs = refs[copies * (ring - 1) : -2]
    own, copy = lax.axis_index("sp"), lax.axis_index("grp")
    half = own_ref.shape[0] // copies
    main = (own_ref.shape[1] - lanes) // 2

    def place_piece(ref, first, source, place):
        start = pl.multiple_of((source * copies + place) * half, half)
        rows = slice(first, first + half)
        for part, weight in enumerate(weights):
            weight[pl.ds(start, half), :main] = ref[rows, part * main : (part + 1) * main]
            weight[pl.ds(start, half), main:] = ref[rows, 2 * main :]

    for place in range(copies):
        place_piece(own_ref, place * half, own, place)
    for step in range(1, ring):
        for turn in range(copies):
            source = lax.rem(own - step + ring, ring)
            place = lax.rem(copy - turn + copies, copies)
            piece = pieces[(step - 1) * copies + turn]
            place_piece(piece, piece.shape[0] - half, source, place)
    count = outs[0].shape[0]
    for index in range(2):
        rows = slice(index * count * ring, (index + 1) * count * ring)
        for part, hidden_ref in enumerate((low_ref, high_ref)):
            units = dot_t(hidden_ref[rows, :], weights[part][...]).astype(jnp.bfloat16)
            for step in range(ring):
                out = outs[index * ring + step]
                for block in range(ring * copies):
                    start = (2 * block + part) * half
                    out[:, start : start + half] = units[
                        step * count : (step + 1) * count, block * half : (block + 1) * half
                    ]


def shards(
    query_rows,
    key_rows,
    value_rows,
    key_logit,
    residual,
    out_weight,
    mix_gain,
    ffn_gain,
    out_gain,
    gate_weight,
    up_weight,
    down_weight,
):
    ring = lax.axis_size("sp")
    copies = lax.axis_size("grp")
    members, member = lax.axis_size("tp"), lax.axis_index("tp")
    tok_rows, width = residual.shape
    own_rows = tok_rows // members
    bits = [1 << i for i in range(members.bit_length() - 1)]
    depth, part = gate_weight.shape[0], gate_weight.shape[1] // ring
    main, share = part // lanes * lanes, depth // copies
    packs = main > 0 and 2 * (part - main) == lanes and ring % 2 == 0 and share % 32 == 0

    attended, packed = attend(query_rows, key_rows, value_rows, key_logit)
    if packs:
        wide, narrow = [None] * ring, [None] * ring
        outer = [step for step in range(1, ring) if step != ring // 2]

        def pack(kernel, rows, *weights):
            shapes = [jax.ShapeDtypeStruct((count, 2 * part), jnp.bfloat16) for count in rows]
            return call(kernel, shapes, 1, *weights)

        gate_in, up_in, _ = lax.optimization_barrier((gate_weight, up_weight, packed))
        pieces = pack(
            functools.partial(pack_outer_kernel, ring, outer),
            [share // 2 * 3] * len(outer),
            gate_in,
            up_in,
            down_weight,
        )
        for step, piece in zip(outer, pieces):
            wide[step] = narrow[step] = exchange(piece, step)
        middle_wide, middle_narrow = pack(
            functools.partial(pack_middle_kernel, ring, ring // 2),
            [share, share // 2],
            gate_weight,
            up_weight,
            down_weight,
        )
        wide[ring // 2] = exchange(middle_wide, ring // 2)
        narrow[ring // 2] = exchange(middle_narrow, ring // 2)
        wide_own, narrow_own = pack(
            functools.partial(pack_own_kernel, ring),
            [depth, depth // 2],
            gate_weight,
            up_weight,
            down_weight,
        )
        wide, narrow = sum(wide[1:], []), sum(narrow[1:], [])

    head_part = jnp.dot(attended, out_weight, preferred_element_type=jnp.float32)
    head_part = head_part.astype(jnp.bfloat16).reshape(members, own_rows, width)
    mixed = jnp.zeros((own_rows, width), jnp.float32)
    for step in range(members):
        piece = lax.dynamic_index_in_dim(head_part, member ^ step, 0, keepdims=False)
        piece = piece if step == 0 else swap(piece, "tp", step)
        mixed = mixed + piece.astype(jnp.float32)
    mixed = mixed.astype(jnp.bfloat16)
    own_residual = lax.dynamic_slice_in_dim(residual, member * own_rows, own_rows, 0)
    middle = (
        own_residual.astype(jnp.float32) + mix_gain * normalize(mixed.astype(jnp.float32))
    ).astype(jnp.bfloat16)
    normed = (ffn_gain * normalize(middle.astype(jnp.float32))).astype(jnp.bfloat16)

    if packs:
        shape = jax.ShapeDtypeStruct
        blocks = {(0, 0): normed}
        for step in range(1, ring):
            blocks[0, step] = shift(normed, "sp", step)
        for bit in reversed(bits):
            for (offset, step), block in list(blocks.items()):
                blocks[offset ^ bit, step] = swap(block, "tp", bit)
        order = [(2 * p + half, k) for half in range(2) for k in range(ring) for p in range(members // 2)]
        all_rows = len(order) * own_rows
        hidden = call(
            functools.partial(wide_kernel, ring, copies, len(order)),
            [shape((all_rows, main + lanes), jnp.bfloat16)] * 2,
            4 * all_rows * width * part,
            *[blocks[key] for key in order],
            wide_own,
            *wide,
            scratch=[
                pltpu.VMEM((width, 2 * part), jnp.bfloat16),
                pltpu.VMEM((all_rows, width), jnp.bfloat16),
            ],
            limit=40 << 20,
        )
        units_out = call(
            functools.partial(narrow_kernel, ring, copies),
            [shape((all_rows // (2 * ring), width), jnp.bfloat16)] * (2 * ring),
            2 * all_rows * width * part,
            *hidden,
            narrow_own,
            *narrow,
            scratch=[pltpu.VMEM((width // 2, main + lanes), jnp.bfloat16)] * 2,
            limit=40 << 20,
        )
        ffn_out = jnp.zeros((own_rows, width), jnp.float32)
        for step in sorted(range(ring), key=lambda k: (k == 0, abs(2 * k - ring))):
            kept, sent = units_out[step], units_out[ring + step]
            sent = swap(sent, "tp", 1)
            units = kept.astype(jnp.float32) + sent.astype(jnp.float32)
            units = units.reshape(members // 2, own_rows, width)
            for bit in bits[1:]:
                moved = swap(units[1::2].astype(jnp.bfloat16), "tp", bit)
                units = units[0::2] + moved.astype(jnp.float32)
            units = units[0]
            if step:
                units = shift(units.astype(jnp.bfloat16), "sp", -step).astype(jnp.float32)
            ffn_out = ffn_out + units
    else:
        gathered = jnp.stack(
            [normed if step == 0 else shift(normed, "sp", step) for step in range(ring)]
        )[None]
        for bit in reversed(bits):
            gathered = jnp.concatenate([gathered, swap(gathered, "tp", bit)], axis=0)
        gathered = gathered.reshape(members * ring * own_rows, width)
        gate_full, up_full, down_full = spread(gate_weight), spread(up_weight), spread(down_weight)
        gate_act = jnp.dot(gathered, gate_full, preferred_element_type=jnp.float32)
        up_act = jnp.dot(gathered, up_full, preferred_element_type=jnp.float32)
        hidden = (jax.nn.silu(gate_act) * up_act).astype(jnp.bfloat16)
        unit_part = lax.dot_general(
            hidden, down_full, (((1,), (1,)), ((), ())), preferred_element_type=jnp.float32
        ).astype(jnp.bfloat16)
        unit_part = unit_part.reshape(members, ring, own_rows, width)
        for bit in bits:
            kept, sent = jnp.split(unit_part, 2, axis=0)
            unit_part = (
                kept.astype(jnp.float32) + swap(sent, "tp", bit).astype(jnp.float32)
            ).astype(jnp.bfloat16)
        ffn_out = unit_part[0, 0].astype(jnp.float32)
        for step in range(1, ring):
            ffn_out = ffn_out + shift(unit_part[0, step], "sp", -step).astype(jnp.float32)
    ffn_out = ffn_out.astype(jnp.bfloat16)
    layer_out = (
        middle.astype(jnp.float32) + out_gain * normalize(ffn_out.astype(jnp.float32))
    ).astype(jnp.bfloat16)
    parts = {0: layer_out}
    for bit in reversed(bits):
        for offset, rows in list(parts.items()):
            parts[offset ^ bit] = swap(rows, "tp", bit)
    result = jnp.zeros((tok_rows, width), jnp.bfloat16)
    for offset in range(members):
        result = lax.dynamic_update_slice(result, parts[offset], ((member ^ offset) * own_rows, 0))
    return result


def solution(mesh):
    placed = (
        P(("grp", "sp"), "tp"),
        P(("grp", "sp"), "tp"),
        P(("grp", "sp"), "tp"),
        P(("grp", "sp"), "tp"),
        P(("grp", "sp"), None),
        P("tp", None),
        P(),
        P(),
        P(),
        P("sp", "tp"),
        P("sp", "tp"),
        P("sp", "tp"),
    )
    return jax.shard_map(
        shards, mesh=mesh, in_specs=placed, out_specs=P(("grp", "sp"), None), check_vma=False
    )
```

```python
import functools
import math

import jax
import jax.numpy as jnp
from jax import lax
from jax.experimental import pallas as pl
from jax.experimental.pallas import tpu as pltpu
from jax.sharding import PartitionSpec as P


epsilon = 1e-06
lanes = 128
pad_rows = 8


def normalize(payload_table):
    return payload_table * lax.rsqrt(
        jnp.mean(payload_table * payload_table, axis=-1, keepdims=True) + epsilon
    )


def shift(rows, axis, step):
    count = lax.axis_size(axis)
    return lax.ppermute(rows, axis, [(i, (i + step) % count) for i in range(count)])


def upward(rows, axis, step):
    count = lax.axis_size(axis)
    return lax.ppermute(rows, axis, [(i, i + step) for i in range(count - step)])


def swap(rows, axis, bit):
    count = lax.axis_size(axis)
    return lax.ppermute(rows, axis, [(i, i ^ bit) for i in range(count)])


def call(kernel, outs, flops, *args, scratch=(), limit=None, outside=0):
    held = [pltpu.with_memory_space_constraint(arg, pltpu.VMEM) for arg in args[outside:]]
    specs = [pl.BlockSpec(memory_space=pltpu.VMEM)] * len(args)
    single = not isinstance(outs, list)
    out_list = [outs] if single else outs
    moved = sum(math.prod(a.shape) * a.dtype.itemsize for a in (*args, *out_list))
    out_specs = [pl.BlockSpec(memory_space=pltpu.VMEM)] * len(out_list)
    return pl.pallas_call(
        kernel,
        out_shape=outs,
        in_specs=specs,
        out_specs=out_specs[0] if single else out_specs,
        scratch_shapes=list(scratch),
        compiler_params=pltpu.CompilerParams(vmem_limit_bytes=limit),
        cost_estimate=pl.CostEstimate(flops=flops, bytes_accessed=moved, transcendentals=0),
    )(*args[:outside], *held)


def dot_t(a, b):
    return lax.dot_general(a, b, (((1,), (1,)), ((), ())), preferred_element_type=jnp.float32)


def pack_kernel(key_ref, value_ref, logit_ref, out_ref):
    tok_rows, width = key_ref.shape
    out_ref[:tok_rows, :width] = key_ref[...]
    out_ref[:tok_rows, width:] = value_ref[...]
    logits = logit_ref[...].astype(jnp.float32)
    rows = [logits, jnp.zeros((pad_rows - logits.shape[0], tok_rows), jnp.float32)]
    out_ref[tok_rows:, :tok_rows] = jnp.concatenate(rows, axis=0).astype(out_ref.dtype)
    out_ref[tok_rows:, tok_rows:] = jnp.zeros((pad_rows, 2 * width - tok_rows), out_ref.dtype)


def attend_kernel(head_count, query_ref, *refs):
    blocks, out_ref = refs[:-1], refs[-1]
    tok_rows, width = query_ref.shape
    head_width = width // head_count
    row = lax.broadcasted_iota(jnp.int32, (tok_rows, tok_rows), 0)
    column = lax.broadcasted_iota(jnp.int32, (tok_rows, tok_rows), 1)
    causal = row > column
    later = causal.astype(jnp.float32).astype(jnp.bfloat16)
    for head in range(head_count):
        own = slice(head * head_width, (head + 1) * head_width)
        queries = query_ref[:, own]
        attended = jnp.zeros((tok_rows, head_width), jnp.float32)
        carried = jnp.zeros((tok_rows, 1), jnp.float32)
        for step, block in enumerate(blocks):
            keys = block[:tok_rows, own]
            values = block[:tok_rows, width + head * head_width : width + (head + 1) * head_width]
            logit = block[tok_rows:, :tok_rows].astype(jnp.float32)[head : head + 1]
            scores = dot_t(queries, keys) * head_width ** (-0.5) + logit
            tail = jnp.log(1.0 + jnp.exp(-jnp.abs(scores)))
            keep_log = -jnp.maximum(scores, 0.0) - tail
            take_log = jnp.minimum(scores, 0.0) - tail
            if step == 0:
                keep_log = jnp.where(causal, keep_log, 0.0)
            high = keep_log.astype(jnp.bfloat16)
            rest = keep_log - high.astype(jnp.float32)
            middle = rest.astype(jnp.bfloat16)
            low = (rest - middle.astype(jnp.float32)).astype(jnp.bfloat16)
            within = (
                jnp.dot(high, later, preferred_element_type=jnp.float32)
                + jnp.dot(middle, later, preferred_element_type=jnp.float32)
                + jnp.dot(low, later, preferred_element_type=jnp.float32)
            )
            sticks = jnp.exp(take_log + within)
            if step == 0:
                sticks = jnp.where(causal, sticks, 0.0)
            partial = jnp.dot(
                sticks.astype(jnp.bfloat16), values, preferred_element_type=jnp.float32
            )
            attended = attended + jnp.exp(carried) * partial
            carried = carried + within[:, :1] + keep_log[:, :1]
        out_ref[:, own] = attended.astype(out_ref.dtype)


def attend(queries, key_part, value_part, logit_part):
    tok_rows, width = queries.shape
    head_count = logit_part.shape[1]
    ring = lax.axis_size("sp")
    packed = call(
        pack_kernel,
        pltpu.VMEM((tok_rows + pad_rows, 2 * width), key_part.dtype),
        1,
        key_part,
        value_part,
        jnp.transpose(logit_part),
        outside=3,
    )
    blocks = [packed] + [upward(packed, "sp", step) for step in range(1, ring)]
    attended = call(
        functools.partial(attend_kernel, head_count),
        jax.ShapeDtypeStruct((tok_rows, width), jnp.bfloat16),
        10 * ring * tok_rows * tok_rows * width,
        queries,
        *blocks,
        outside=1,
    )
    return attended, packed


def spread(weight):
    ring, own = lax.axis_size("sp"), lax.axis_index("sp")
    copies, copy = lax.axis_size("grp"), lax.axis_index("grp")
    rows, columns = weight.shape
    part, share = columns // ring, rows // copies
    pieces = weight.reshape(rows, ring, part).transpose(1, 0, 2)
    result = jnp.zeros((ring * rows, part), weight.dtype)
    mine = lax.dynamic_index_in_dim(pieces, own, 0, keepdims=False)
    result = lax.dynamic_update_slice(result, mine, (own * rows, 0))
    for step in range(1, ring):
        target, source = (own + step) % ring, (own - step) % ring
        piece = lax.dynamic_slice(pieces, (target, copy * share, 0), (1, share, part))[0]
        piece = shift(piece, "sp", step)
        for turn in range(copies):
            other = piece if turn == 0 else shift(piece, "grp", turn)
            place = (copy - turn) % copies
            result = lax.dynamic_update_slice(result, other, (source * rows + place * share, 0))
    return result


def tile_at(ref, rows, ring, target):
    main = ref.shape[1] // ring // lanes * lanes
    start = pl.multiple_of(ring * main + target // 2 * lanes, lanes)
    return ref[rows, pl.ds(start, lanes)].astype(jnp.float32)


def main_at(ref, rows, ring, target):
    main = ref.shape[1] // ring // lanes * lanes
    return ref[rows, pl.ds(pl.multiple_of(target * main, lanes), main)]


def halves(low, high, odd):
    lower = lax.broadcasted_iota(jnp.int32, low.shape, 1) < lanes // 2
    low = jnp.where(odd, pltpu.roll(low, lanes // 2, 1), low)
    high = jnp.where(odd, high, pltpu.roll(high, lanes // 2, 1))
    return jnp.where(lower, low, high).astype(jnp.bfloat16)


def pack_wide(out, gate_ref, up_ref, rows, ring, target):
    gate, up = main_at(gate_ref, rows, ring, target), main_at(up_ref, rows, ring, target)
    count, main = gate.shape
    out[:count, :main] = gate
    out[:count, main : 2 * main] = up
    out[:count, 2 * main :] = halves(
        tile_at(gate_ref, rows, ring, target),
        tile_at(up_ref, rows, ring, target),
        target % 2 == 1,
    )


def pack_narrow(out, place, down_ref, start, half, ring, target):
    upper = pl.ds(pl.multiple_of(start, half), half)
    lower = pl.ds(pl.multiple_of(start + half, half), half)
    main = (out.shape[1] - lanes) // 2
    rows = slice(place, place + half)
    out[rows, :main] = main_at(down_ref, upper, ring, target)
    out[rows, main : 2 * main] = main_at(down_ref, lower, ring, target)
    out[rows, 2 * main :] = halves(
        tile_at(down_ref, upper, ring, target),
        tile_at(down_ref, lower, ring, target),
        target % 2 == 1,
    )


def pack_outer_kernel(ring, steps, gate_ref, up_ref, down_ref, *out_refs):
    own, copy = lax.axis_index("sp"), lax.axis_index("grp")
    for step, out in zip(steps, out_refs):
        share = out.shape[0] // 3 * 2
        target = lax.rem(own + step, ring)
        start = pl.multiple_of(copy * share, share)
        pack_wide(out, gate_ref, up_ref, pl.ds(start, share), ring, target)
        pack_narrow(out, share, down_ref, start, share // 2, ring, target)


def pack_middle_kernel(ring, step, gate_ref, up_ref, down_ref, wide_ref, narrow_ref):
    own, copy = lax.axis_index("sp"), lax.axis_index("grp")
    share = wide_ref.shape[0]
    target = lax.rem(own + step, ring)
    start = pl.multiple_of(copy * share, share)
    pack_wide(wide_ref, gate_ref, up_ref, pl.ds(start, share), ring, target)
    pack_narrow(narrow_ref, 0, down_ref, start, share // 2, ring, target)


def pack_own_kernel(ring, gate_ref, up_ref, down_ref, wide_ref, narrow_ref):
    own = lax.axis_index("sp")
    share = wide_ref.shape[0] // lax.axis_size("grp")
    pack_wide(wide_ref, gate_ref, up_ref, slice(None), ring, own)
    for copy in range(lax.axis_size("grp")):
        place = copy * share // 2
        pack_narrow(narrow_ref, place, down_ref, copy * share, share // 2, ring, own)


def exchange(piece, step):
    piece = shift(piece, "sp", step)
    turns = range(1, lax.axis_size("grp"))
    return [piece] + [shift(piece, "grp", turn) for turn in turns]


def wide_kernel(ring, copies, block_count, *refs):
    blocks, refs = refs[:block_count], refs[block_count:]
    own_ref, pieces, (low_ref, high_ref), scratch = refs[0], refs[1:-4], refs[-4:-2], refs[-2:]
    weight, rows_ref = scratch
    own, copy = lax.axis_index("sp"), lax.axis_index("grp")
    block_rows = blocks[0].shape[0]
    for index, block in enumerate(blocks):
        rows_ref[index * block_rows : (index + 1) * block_rows, :] = block[...]
    depth, share = own_ref.shape[0], own_ref.shape[0] // copies
    weight[pl.ds(pl.multiple_of(own * depth, depth), depth), :] = own_ref[...]
    for step in range(1, ring):
        for turn in range(copies):
            source = lax.rem(own - step + ring, ring)
            place = lax.rem(copy - turn + copies, copies)
            start = pl.multiple_of(source * depth + place * share, share)
            weight[pl.ds(start, share), :] = pieces[(step - 1) * copies + turn][:share]
    main = (own_ref.shape[1] - lanes) // 2
    count = rows_ref.shape[0]
    tile = min(count, 512)

    def body(index, _):
        rows = pl.ds(pl.multiple_of(index * tile, tile), tile)
        block = rows_ref[rows, :]
        gate = jnp.dot(block, weight[:, :main], preferred_element_type=jnp.float32)
        up = jnp.dot(block, weight[:, main : 2 * main], preferred_element_type=jnp.float32)
        both = jnp.dot(block, weight[:, 2 * main :], preferred_element_type=jnp.float32)
        hidden = (gate / (1.0 + jnp.exp(-gate)) * up).astype(jnp.bfloat16)
        rest = both / (1.0 + jnp.exp(-both)) * pltpu.roll(both, lanes // 2, 1)
        lower = lax.broadcasted_iota(jnp.int32, rest.shape, 1) < lanes // 2
        rest = jnp.where(lower, rest, 0.0)
        low_ref[rows, :main] = hidden
        high_ref[rows, :main] = hidden
        low_ref[rows, main:] = rest.astype(jnp.bfloat16)
        high_ref[rows, main:] = pltpu.roll(rest, lanes // 2, 1).astype(jnp.bfloat16)
        return 0

    lax.fori_loop(0, count // tile, body, 0)


def narrow_kernel(ring, copies, low_ref, high_ref, own_ref, *refs):
    pieces, weights = refs[: copies * (ring - 1)], refs[-2:]
    outs = refs[copies * (ring - 1) : -2]
    own, copy = lax.axis_index("sp"), lax.axis_index("grp")
    half = own_ref.shape[0] // copies
    main = (own_ref.shape[1] - lanes) // 2

    def place_piece(ref, first, source, place):
        start = pl.multiple_of((source * copies + place) * half, half)
        rows = slice(first, first + half)
        for part, weight in enumerate(weights):
            weight[pl.ds(start, half), :main] = ref[rows, part * main : (part + 1) * main]
            weight[pl.ds(start, half), main:] = ref[rows, 2 * main :]

    for place in range(copies):
        place_piece(own_ref, place * half, own, place)
    for step in range(1, ring):
        for turn in range(copies):
            source = lax.rem(own - step + ring, ring)
            place = lax.rem(copy - turn + copies, copies)
            piece = pieces[(step - 1) * copies + turn]
            place_piece(piece, piece.shape[0] - half, source, place)
    count = outs[0].shape[0]
    for index in range(2):
        rows = slice(index * count * ring, (index + 1) * count * ring)
        for part, hidden_ref in enumerate((low_ref, high_ref)):
            units = dot_t(hidden_ref[rows, :], weights[part][...]).astype(jnp.bfloat16)
            for step in range(ring):
                out = outs[index * ring + step]
                for block in range(ring * copies):
                    start = (2 * block + part) * half
                    out[:, start : start + half] = units[
                        step * count : (step + 1) * count, block * half : (block + 1) * half
                    ]


def shards(
    query_rows,
    key_rows,
    value_rows,
    key_logit,
    residual,
    out_weight,
    mix_gain,
    ffn_gain,
    out_gain,
    gate_weight,
    up_weight,
    down_weight,
):
    ring = lax.axis_size("sp")
    copies = lax.axis_size("grp")
    members, member = lax.axis_size("tp"), lax.axis_index("tp")
    tok_rows, width = residual.shape
    own_rows = tok_rows // members
    bits = [1 << i for i in range(members.bit_length() - 1)]
    depth, part = gate_weight.shape[0], gate_weight.shape[1] // ring
    main, share = part // lanes * lanes, depth // copies
    packs = main > 0 and 2 * (part - main) == lanes and ring % 2 == 0 and share % 32 == 0

    attended, packed = attend(query_rows, key_rows, value_rows, key_logit)
    if packs:
        wide, narrow = [None] * ring, [None] * ring
        outer = [step for step in range(1, ring) if step != ring // 2]

        def pack(kernel, rows, *weights):
            shapes = [pltpu.VMEM((count, 2 * part), jnp.bfloat16) for count in rows]
            return call(kernel, shapes, 1, *weights, outside=len(weights))

        gate_in, up_in, _ = lax.optimization_barrier((gate_weight, up_weight, packed))
        pieces = pack(
            functools.partial(pack_outer_kernel, ring, outer),
            [share // 2 * 3] * len(outer),
            gate_in,
            up_in,
            down_weight,
        )
        for step, piece in zip(outer, pieces):
            wide[step] = narrow[step] = exchange(piece, step)
        middle_wide, middle_narrow = pack(
            functools.partial(pack_middle_kernel, ring, ring // 2),
            [share, share // 2],
            gate_weight,
            up_weight,
            down_weight,
        )
        wide[ring // 2] = exchange(middle_wide, ring // 2)
        narrow[ring // 2] = exchange(middle_narrow, ring // 2)
        wide_own, narrow_own = pack(
            functools.partial(pack_own_kernel, ring),
            [depth, depth // 2],
            gate_weight,
            up_weight,
            down_weight,
        )
        wide, narrow = sum(wide[1:], []), sum(narrow[1:], [])

    head_part = jnp.dot(attended, out_weight, preferred_element_type=jnp.float32)
    head_part = head_part.astype(jnp.bfloat16).reshape(members, own_rows, width)
    mixed = jnp.zeros((own_rows, width), jnp.float32)
    for step in range(members):
        piece = lax.dynamic_index_in_dim(head_part, member ^ step, 0, keepdims=False)
        piece = piece if step == 0 else swap(piece, "tp", step)
        mixed = mixed + piece.astype(jnp.float32)
    mixed = mixed.astype(jnp.bfloat16)
    own_residual = lax.dynamic_slice_in_dim(residual, member * own_rows, own_rows, 0)
    middle = (
        own_residual.astype(jnp.float32) + mix_gain * normalize(mixed.astype(jnp.float32))
    ).astype(jnp.bfloat16)
    normed = (ffn_gain * normalize(middle.astype(jnp.float32))).astype(jnp.bfloat16)

    if packs:
        shape = jax.ShapeDtypeStruct
        blocks = {(0, 0): normed}
        for step in range(1, ring):
            blocks[0, step] = shift(normed, "sp", step)
        for bit in reversed(bits):
            for (offset, step), block in list(blocks.items()):
                blocks[offset ^ bit, step] = swap(block, "tp", bit)
        order = [(2 * p + half, k) for half in range(2) for k in range(ring) for p in range(members // 2)]
        all_rows = len(order) * own_rows
        hidden = call(
            functools.partial(wide_kernel, ring, copies, len(order)),
            [shape((all_rows, main + lanes), jnp.bfloat16)] * 2,
            4 * all_rows * width * part,
            *[blocks[key] for key in order],
            wide_own,
            *wide,
            scratch=[
                pltpu.VMEM((width, 2 * part), jnp.bfloat16),
                pltpu.VMEM((all_rows, width), jnp.bfloat16),
            ],
            limit=40 << 20,
        )
        units_out = call(
            functools.partial(narrow_kernel, ring, copies),
            [shape((all_rows // (2 * ring), width), jnp.bfloat16)] * (2 * ring),
            2 * all_rows * width * part,
            *hidden,
            narrow_own,
            *narrow,
            scratch=[pltpu.VMEM((width // 2, main + lanes), jnp.bfloat16)] * 2,
            limit=40 << 20,
        )
        ffn_out = jnp.zeros((own_rows, width), jnp.float32)
        for step in sorted(range(ring), key=lambda k: (k == 0, abs(2 * k - ring))):
            kept, sent = units_out[step], units_out[ring + step]
            sent = swap(sent, "tp", 1)
            units = kept.astype(jnp.float32) + sent.astype(jnp.float32)
            units = units.reshape(members // 2, own_rows, width)
            for bit in bits[1:]:
                moved = swap(units[1::2].astype(jnp.bfloat16), "tp", bit)
                units = units[0::2] + moved.astype(jnp.float32)
            units = units[0]
            if step:
                units = shift(units.astype(jnp.bfloat16), "sp", -step).astype(jnp.float32)
            ffn_out = ffn_out + units
    else:
        gathered = jnp.stack(
            [normed if step == 0 else shift(normed, "sp", step) for step in range(ring)]
        )[None]
        for bit in reversed(bits):
            gathered = jnp.concatenate([gathered, swap(gathered, "tp", bit)], axis=0)
        gathered = gathered.reshape(members * ring * own_rows, width)
        gate_full, up_full, down_full = spread(gate_weight), spread(up_weight), spread(down_weight)
        gate_act = jnp.dot(gathered, gate_full, preferred_element_type=jnp.float32)
        up_act = jnp.dot(gathered, up_full, preferred_element_type=jnp.float32)
        hidden = (jax.nn.silu(gate_act) * up_act).astype(jnp.bfloat16)
        unit_part = lax.dot_general(
            hidden, down_full, (((1,), (1,)), ((), ())), preferred_element_type=jnp.float32
        ).astype(jnp.bfloat16)
        unit_part = unit_part.reshape(members, ring, own_rows, width)
        for bit in bits:
            kept, sent = jnp.split(unit_part, 2, axis=0)
            unit_part = (
                kept.astype(jnp.float32) + swap(sent, "tp", bit).astype(jnp.float32)
            ).astype(jnp.bfloat16)
        ffn_out = unit_part[0, 0].astype(jnp.float32)
        for step in range(1, ring):
            ffn_out = ffn_out + shift(unit_part[0, step], "sp", -step).astype(jnp.float32)
    ffn_out = ffn_out.astype(jnp.bfloat16)
    layer_out = (
        middle.astype(jnp.float32) + out_gain * normalize(ffn_out.astype(jnp.float32))
    ).astype(jnp.bfloat16)
    parts = {0: layer_out}
    for bit in reversed(bits):
        for offset, rows in list(parts.items()):
            parts[offset ^ bit] = swap(rows, "tp", bit)
    result = jnp.zeros((tok_rows, width), jnp.bfloat16)
    for offset in range(members):
        result = lax.dynamic_update_slice(result, parts[offset], ((member ^ offset) * own_rows, 0))
    return result


def solution(mesh):
    placed = (
        P(("grp", "sp"), "tp"),
        P(("grp", "sp"), "tp"),
        P(("grp", "sp"), "tp"),
        P(("grp", "sp"), "tp"),
        P(("grp", "sp"), None),
        P("tp", None),
        P(),
        P(),
        P(),
        P("sp", "tp"),
        P("sp", "tp"),
        P("sp", "tp"),
    )
    return jax.shard_map(
        shards, mesh=mesh, in_specs=placed, out_specs=P(("grp", "sp"), None), check_vma=False
    )
```
